32 devices in a mesh: ep: 8 (over z, y), tp: 4 (over x, core).
Axes of the slice: x: 2, y: 2, z: 4, core: 2. Of those that a mesh axis runs over, the one named last changes fastest.
Arguments:
- q_heads: bfloat16 [8192, 1024], P('ep', 'tp'), may hold values from -200 to 200
- k_heads: bfloat16 [8192, 256], P('ep', 'tp'), may hold values from -6 to 6
- v_heads: bfloat16 [8192, 256], P('ep', 'tp'), may hold values from -6 to 6
- sink_logits: float32 [16], P('tp'), may hold values from 1 to 5
- out_weight: bfloat16 [1024, 2048], P(None, 'tp'), may hold values from -1.5 to 1.5
- tokens_b: bfloat16 [4096, 2048], P('ep'), may hold values from -6 to 6
- moe_gain: float32 [2048], replicated, may hold values from 0.1 to 1.9
- router_group: bfloat16 [2048, 4], replicated, may hold values from -0.125 to 0.125
- router_expert: bfloat16 [2048, 16], replicated, may hold values from -0.125 to 0.125
- route_expert: int32 [4096, 2], P('ep'), may hold values from 0 to 15, as said below
- expert_gate: bfloat16 [16, 2048, 1024], P('ep', None, 'tp'), may hold values from -0.125 to 0.125
- expert_up: bfloat16 [16, 2048, 1024], P('ep', None, 'tp'), may hold values from -0.125 to 0.125
- expert_down: bfloat16 [16, 1024, 2048], P('ep', 'tp'), may hold values from -0.75 to 0.75
Outputs:
- mixer_out: bfloat16 [8192, 2048], P('ep', 'tp')
- moe_out: bfloat16 [4096, 2048], P(('ep', 'tp'))
The draws below stay inside these ranges and needn't reach their ends.
Inputs may be any that keep to these rules, and one draw needn't show every extreme that they name: `route_expert`: each token names two different experts, in rising order, of one group of 4 consecutive experts. In each aligned block of 128 rows (the rows of one device) no expert is named by more than 32 tokens, in each group one expert is named by exactly 32 tokens of every block, and each group is named by a quarter of every block's tokens.
All inputs are finite; a program needn't handle non-finite values.
Results may differ from the reference program's by a relative error of at most 0.011.
Values may be sent and summed in bfloat16 or wider, within the bound.
A program may use at most 128 MiB of HBM per device.

```python
import jax
import jax.numpy as jnp
from jax import lax

D = 2048
HEADS = 16
KV = 4
HD = 64
WINDOW = 128
ROW_B = 128
GROUPS = 4
FF = 1024
EXPERTS = 16
GROUP_EXPERTS = 4
CAP = 32
TOK_A = 8192
TOK_B = 4096
N_EP = 8
N_TP = 4


def pair_heads(seed_key):
    key_query, key_keys = jax.random.split(seed_key, 2)
    group_size = HEADS // KV
    queries = jnp.clip(jax.random.normal(key_query, (TOK_A, KV, group_size, HD), jnp.float32), -5.0, 5.0)
    keys_raw = jnp.clip(jax.random.normal(key_keys, (TOK_A, KV, HD), jnp.float32), -5.0, 5.0)
    return (queries.reshape(TOK_A, HEADS * HD), keys_raw.reshape(TOK_A, KV * HD))


def draw_q_heads(key, part):
    return pair_heads(jax.random.fold_in(key, 3))[0].astype(jnp.bfloat16)


def draw_k_heads(key, part):
    return pair_heads(jax.random.fold_in(key, 3))[1].astype(jnp.bfloat16)


def draw_route_expert(key, part):
    block_count = N_EP * N_TP
    half_rows = ROW_B // 2
    quarter_rows = ROW_B // 4
    pool = jnp.repeat(jnp.arange(GROUP_EXPERTS, dtype=jnp.int32), CAP)
    favored = jax.random.randint(jax.random.fold_in(key, 7), (GROUPS,), 0, GROUP_EXPERTS)

    def one_group(group_key, group_index):
        ranks = jax.random.permutation(group_key, pool.shape[0]).astype(jnp.int32)
        ordering = jnp.where(pool == favored[group_index], -1, ranks)
        order = jnp.argsort(ordering, stable=True)
        picked = jnp.sort(pool[order[:half_rows]])
        pairs = jnp.stack([picked[:quarter_rows], picked[quarter_rows:]], axis=1)
        return pairs + group_index * GROUP_EXPERTS

    def one_block(block_key):
        group_keys = jax.random.split(block_key, GROUPS + 1)
        pairs = jax.vmap(one_group)(group_keys[:GROUPS], jnp.arange(GROUPS, dtype=jnp.int32))
        pairs = pairs.reshape(ROW_B, 2)
        return pairs[jax.random.permutation(group_keys[GROUPS], ROW_B)]
    block_keys = jax.random.split(jax.random.fold_in(key, 11), block_count)
    return jax.vmap(one_block)(block_keys).reshape(block_count * ROW_B, 2).astype(jnp.int32)


def block_levels(own_key, dims, cuts, low, largest):
    loudness, own = 1.0, jax.random.fold_in(own_key, 6)
    for axis_at, shards_of in cuts:
        heights = jnp.exp(jax.random.uniform(jax.random.fold_in(own, axis_at), (shards_of,), jnp.float32, low / len(cuts), largest / len(cuts)))
        loudness = loudness * jnp.repeat(heights, dims[axis_at] // shards_of).reshape([-1 if axis == axis_at else 1 for axis in range(len(dims))])
    return loudness


def scatter_about(key, dims, spread, limit, cuts=(), held_as=jnp.bfloat16):
    result = spread * jax.random.normal(key, dims, jnp.float32)
    if cuts:
        result = result * block_levels(key, dims, cuts, -0.22, 0.18)
    return jnp.clip(result, -limit, limit).astype(held_as)


def setup_inputs(seed: int = 0) -> dict:
    key_of = jax.random.split(jax.random.key(seed), 14)
    q_heads = draw_q_heads(jax.random.fold_in(key_of[13], 71), 0)
    k_heads = draw_k_heads(jax.random.fold_in(key_of[13], 71), 0)
    v_heads = scatter_about(key_of[2], (TOK_A, KV * HD), 1.0, 6.0, ((0, 8), (1, 4)))
    sink_logits = jnp.clip(1.0 + 4.0 * jax.random.uniform(key_of[3], (HEADS,), jnp.float32) ** block_levels(key_of[3], (HEADS,), ((0, 4),), -0.2, 0.2), 1.0, 5.0)
    out_weight = scatter_about(key_of[4], (HEADS * HD, D), HEADS ** -0.5, 1.5, ((1, 4),))
    tokens_b = scatter_about(key_of[5], (TOK_B, D), 1.0, 6.0, ((0, 8),))
    moe_gain = jnp.clip(1.0 + 0.18 * jax.random.normal(key_of[6], (D,), jnp.float32), 0.1, 1.9)
    router_group = scatter_about(key_of[7], (D, GROUPS), D ** -0.5, 0.125)
    router_expert = scatter_about(key_of[8], (D, EXPERTS), D ** -0.5, 0.125)
    route_expert = draw_route_expert(jax.random.fold_in(key_of[13], 71), 0)
    expert_gate = scatter_about(key_of[10], (EXPERTS, D, FF), D ** -0.5, 0.125, ((0, 8), (2, 4)))
    expert_up = scatter_about(key_of[11], (EXPERTS, D, FF), D ** -0.5, 0.125, ((0, 8), (2, 4)))
    expert_down = scatter_about(key_of[12], (EXPERTS, FF, D), (FF // 16) ** -0.5, 0.75, ((0, 8), (1, 4)))
    return {"q_heads": q_heads, "k_heads": k_heads, "v_heads": v_heads, "sink_logits": sink_logits, "out_weight": out_weight, "tokens_b": tokens_b, "moe_gain": moe_gain, "router_group": router_group, "router_expert": router_expert, "route_expert": route_expert, "expert_gate": expert_gate, "expert_up": expert_up, "expert_down": expert_down}


def banded(values, blocks, span_len):
    shaped = values.reshape(TOK_A, KV, HD)
    padded = jnp.concatenate([jnp.zeros((span_len, KV, HD), shaped.dtype), shaped], axis=0)
    padded = padded.reshape(blocks + 1, span_len, KV, HD)
    band = jnp.concatenate([padded[:-1], padded[1:]], axis=1)
    return jnp.moveaxis(band, 2, 0)

def gate_weights(normed, routes, router_group, router_expert):
    group_logits = jnp.dot(normed, router_group, preferred_element_type=jnp.float32)
    expert_logits = jnp.dot(normed, router_expert, preferred_element_type=jnp.float32)
    group_count = router_group.shape[1]
    expert_count = router_expert.shape[1]
    chosen_group = routes[:, 0] // (expert_count // group_count)
    group_match = chosen_group[:, None] == jnp.arange(group_count, dtype=jnp.int32)[None, :]
    group_share = lax.optimization_barrier(jnp.sum(jnp.where(group_match, jax.nn.softmax(group_logits, axis=-1), 0.0), axis=-1))
    expert_match = routes[:, :, None] == jnp.arange(expert_count, dtype=jnp.int32)[None, None, :]
    picked = lax.optimization_barrier(jnp.sum(jnp.where(expert_match, expert_logits[:, None, :], 0.0), axis=-1))
    return group_share[:, None] * jax.nn.softmax(picked, axis=-1)

def reference(q_heads, k_heads, v_heads, sink_logits, out_weight, tokens_b, moe_gain, router_group, router_expert, route_expert, expert_gate, expert_up, expert_down):
    span_len = WINDOW
    blocks = TOK_A // span_len
    group_size = HEADS // KV
    query_blocks = jnp.moveaxis(q_heads.reshape(blocks, span_len, KV, group_size, HD), 2, 0)
    key_band = banded(k_heads, blocks, span_len)
    value_band = banded(v_heads, blocks, span_len)
    query_index = jnp.arange(span_len, dtype=jnp.int32)[:, None]
    key_index = jnp.arange(2 * span_len, dtype=jnp.int32)[None, :]
    distance = query_index + span_len - key_index
    key_place = jnp.arange(blocks, dtype=jnp.int32)[:, None, None] * span_len + key_index[None] - span_len
    allowed = (distance >= 0)[None] & (distance < span_len)[None] & (key_place >= 0)
    sink_rows = sink_logits.reshape(KV, group_size)

    def one_head(packed):
        query_block, key_rows, value_rows, sink_row = packed
        scores = jnp.einsum('nqgd,nkd->ngqk', query_block.astype(jnp.float32), key_rows.astype(jnp.float32)) * HD ** (-0.5)
        masked = jnp.where(allowed[:, None], scores, -1e+30)
        sink_full = sink_row[None, :, None]
        row_max = jnp.maximum(lax.optimization_barrier(jnp.max(masked, axis=-1)), sink_full)
        weights_exp = jnp.exp(masked - row_max[..., None])
        denominator = lax.optimization_barrier(jnp.sum(weights_exp, axis=-1)) + jnp.exp(sink_full - row_max)
        probs = lax.optimization_barrier((weights_exp / denominator[..., None]).astype(jnp.bfloat16))
        mixed = jnp.einsum('ngqk,nkd->nqgd', probs.astype(jnp.float32), value_rows.astype(jnp.float32))
        return mixed.astype(jnp.bfloat16)
    attended = lax.map(one_head, (query_blocks, key_band, value_band, sink_rows))
    attended = jnp.moveaxis(attended, 0, 2).reshape(TOK_A, HEADS * HD)
    mixer_out = jnp.dot(attended, out_weight, preferred_element_type=jnp.float32).astype(jnp.bfloat16)
    blocks_b = N_EP * N_TP
    values = tokens_b.astype(jnp.float32)
    normed = (values * lax.rsqrt(lax.optimization_barrier(jnp.mean(values * values, axis=-1, keepdims=True)) + 1e-06) * moe_gain).astype(jnp.bfloat16)
    gates = gate_weights(normed, route_expert, router_group, router_expert)
    flat_routes = route_expert.reshape(blocks_b, 2 * ROW_B)
    onehot = (flat_routes[:, :, None] == jnp.arange(EXPERTS, dtype=jnp.int32)[None, None, :]).astype(jnp.int32)
    places = lax.optimization_barrier(jnp.sum(onehot * jnp.cumsum(onehot, axis=1), axis=2)) - 1
    token_ids = (jnp.arange(TOK_B * 2, dtype=jnp.int32) // 2).reshape(blocks_b, 2 * ROW_B)
    block_ids = jnp.broadcast_to(jnp.arange(blocks_b, dtype=jnp.int32)[:, None], (blocks_b, 2 * ROW_B))
    slot_token = jnp.full((EXPERTS, blocks_b, CAP), TOK_B, jnp.int32).at[flat_routes, block_ids, places].set(token_ids)
    slot_gate = jnp.zeros((EXPERTS, blocks_b, CAP), jnp.float32).at[flat_routes, block_ids, places].set(gates.reshape(blocks_b, 2 * ROW_B))
    padded_rows = jnp.concatenate([normed, jnp.zeros((1, D), jnp.bfloat16)], axis=0)
    hidden_block = FF // N_TP

    def one_expert(running, packed):
        token_list, gate_list, w_gate, w_up, w_down = packed
        rows_in = padded_rows[token_list]
        gate_pre = jnp.dot(rows_in, w_gate, preferred_element_type=jnp.float32)
        up_pre = jnp.dot(rows_in, w_up, preferred_element_type=jnp.float32)
        activated = lax.optimization_barrier((jax.nn.silu(gate_pre) * up_pre).astype(jnp.bfloat16))
        pieces = jnp.einsum('ntf,tfd->ntd', activated.reshape(-1, N_TP, hidden_block).astype(jnp.float32), w_down.reshape(N_TP, hidden_block, D).astype(jnp.float32))
        pieces = lax.optimization_barrier(pieces.astype(jnp.bfloat16)).astype(jnp.float32)
        expert_out = lax.optimization_barrier(lax.optimization_barrier(jnp.sum(pieces, axis=1)).astype(jnp.bfloat16)).astype(jnp.float32)
        running = running.at[token_list].add(gate_list[:, None] * expert_out)
        return (running, None)
    running = jnp.zeros((TOK_B + 1, D), jnp.float32)
    running, _ = lax.scan(one_expert, running, (slot_token.reshape(EXPERTS, -1), slot_gate.reshape(EXPERTS, -1), expert_gate, expert_up, expert_down))
    moe_out = running[:TOK_B].astype(jnp.bfloat16)
    return (mixer_out, moe_out)
```

```python
import functools

import jax
import jax.numpy as jnp
from jax import lax
from jax.experimental import pallas as pl
from jax.experimental.pallas import tpu as pltpu
from jax.sharding import PartitionSpec as P

HEADS = 16
KV = 4
HD = 64
WINDOW = 128


def shifted(value, axis, steps):
    count = lax.axis_size(axis)
    leading, last = (max(0, -steps), min(count, count - steps))
    return lax.ppermute(value, axis, [(source, source + steps) for source in range(leading, last)])


def normalize(rows_in, gain):
    values = rows_in.astype(jnp.float32)
    scaled = values * lax.rsqrt(jnp.mean(values * values, axis=-1, keepdims=True) + 1e-06) * gain
    return scaled.astype(jnp.bfloat16)


def gate_weights(normed, routes, router_group, router_expert):
    group_logits = jnp.dot(normed, router_group, preferred_element_type=jnp.float32)
    expert_logits = jnp.dot(normed, router_expert, preferred_element_type=jnp.float32)
    group_count = router_group.shape[1]
    expert_count = router_expert.shape[1]
    chosen_group = routes[:, 0] // (expert_count // group_count)
    group_match = chosen_group[:, None] == jnp.arange(group_count, dtype=jnp.int32)[None, :]
    group_share = jnp.sum(
        jnp.where(group_match, jax.nn.softmax(group_logits, axis=-1), 0.0), axis=-1
    )
    expert_match = routes[:, :, None] == jnp.arange(expert_count, dtype=jnp.int32)[None, None, :]
    picked = jnp.sum(jnp.where(expert_match, expert_logits[:, None, :], 0.0), axis=-1)
    return group_share[:, None] * jax.nn.softmax(picked, axis=-1)


def slot_positions(routes, sub_count, expert_count):
    flat_routes = routes.reshape(sub_count, -1)
    onehot = (
        flat_routes[:, :, None] == jnp.arange(expert_count, dtype=jnp.int32)[None, None, :]
    ).astype(jnp.int32)
    places = jnp.sum(onehot * jnp.cumsum(onehot, axis=1), axis=2) - 1
    return (flat_routes, places)


def fill_slots(normed, flat_routes, places, sub_count, expert_count, capacity, exp_local):
    sub_index = jnp.arange(sub_count, dtype=jnp.int32)[:, None]
    target = ((flat_routes * sub_count + sub_index) * capacity + places).reshape(-1)
    source = jnp.repeat(normed, 2, axis=0)
    buffer = jnp.zeros((expert_count * sub_count * capacity, normed.shape[1]), jnp.bfloat16)
    buffer = buffer.at[target].set(source)
    return buffer.reshape(
        expert_count // exp_local, exp_local, sub_count, capacity, normed.shape[1]
    )


LANES = 128
MESH = pl.DeviceIdType.MESH
NS = jax.named_scope
FIRST = "0"
SENDERS = 24
RECEIVERS = 52


def UNITS(chunk):
    half = chunk // 2
    return {
        "0": (0, 0, chunk),
        "1": (1, 0, chunk),
        "2": (2, 0, chunk),
        "a": (3, 0, half),
        "b": (3, half, half),
    }


def fused_kernel(
    groups,
    sink_hbm,
    q_hbm,
    k_hbm,
    v_hbm,
    gain_hbm,
    group_hbm,
    expert_hbm,
    route_hbm,
    tokens_hbm,
    gate_hbm,
    up_hbm,
    down_hbm,
    proj_hbm,
    mixer_hbm,
    out_hbm,
    sink_ref,
    q_ref,
    gain_ref,
    group_ref,
    expert_ref,
    route_ref,
    k_ext,
    v_ext,
    tokens,
    xs_ref,
    heads,
    rows,
    part,
    wg,
    wu,
    wd,
    proj,
    act,
    from_core,
    relay_x,
    relay_y,
    from_xy,
    total,
    back,
    mixed,
    moved,
    load_sem,
    out_sem,
    send_sem,
    recv_sem,
):
    ep, tp = lax.axis_index("ep"), lax.axis_index("tp")
    group, member = ep // 2, ep % 2
    x, core = tp // 2, tp % 2
    tp_x, tp_c = (1 - x) * 2 + core, x * 2 + (1 - core)
    ep_y = group * 2 + (1 - member)
    ep_count = groups * 2
    x_dev, y_dev, c_dev = (ep, tp_x), (ep_y, tp), (ep, tp_c)
    next_dev = ((ep + 1) % ep_count, tp)
    prev_dev = ((ep + ep_count - 1) % ep_count, tp)
    depth = back.shape[1]
    block = xs_ref.shape[0]
    chunk = block // groups
    row_count = q_ref.shape[0]
    mine, other = core * 4, (1 - core) * 4
    own = mine + member * 2 + x
    slot_x = mine + member * 2 + (1 - x)
    slot_y = mine + (1 - member) * 2 + x
    slot_d = mine + (1 - member) * 2 + (1 - x)
    mine_slots, other_slots = pl.ds(mine, 4), pl.ds(other, 4)

    def plane(step):
        return (group + step) % groups

    barrier = pltpu.get_barrier_semaphore()
    ahead = [plane(step) * 2 + member for step in range(1, groups)]
    peers = [(there, tp) for there in ahead] + [x_dev, y_dev, c_dev, next_dev, prev_dev]
    for peer in peers:
        pl.semaphore_signal(barrier, inc=1, device_id=peer, device_id_type=MESH)

    first = pl.multiple_of(tp * block, block)
    inner = pl.ds(WINDOW, row_count)
    pairs = (
        (tokens_hbm.at[pl.ds(first, block)], tokens),
        (gain_hbm, gain_ref),
        (group_hbm, group_ref),
        (expert_hbm, expert_ref),
        (route_hbm.at[:, pl.ds(first, block)], route_ref),
        (k_hbm, k_ext.at[:, inner]),
        (v_hbm, v_ext.at[:, inner]),
        (q_hbm, q_ref),
        (sink_hbm, sink_ref),
        (gate_hbm, wg),
        (up_hbm, wu),
        (down_hbm, wd),
        (proj_hbm, proj),
    )
    loads = [
        pltpu.make_async_copy(source, held, load_sem.at[i])
        for i, (source, held) in enumerate(pairs)
    ]
    early, middle, late = loads[:5], loads[5:9], loads[9:]
    for load in early + middle:
        load.start()
    with NS("wearly"):
        for load in early:
            load.wait()
    for load in late:
        load.start()
    values = tokens[...].astype(jnp.float32)
    scale = lax.rsqrt(jnp.mean(values * values, axis=1, keepdims=True) + 1e-06)
    normed = (values * scale * gain_ref[...]).astype(jnp.bfloat16)
    across = (((1,), (1,)), ((), ()))
    group_logits = lax.dot_general(
        group_ref[...], normed, across, preferred_element_type=jnp.float32
    )
    expert_logits = lax.dot_general(
        expert_ref[...], normed, across, preferred_element_type=jnp.float32
    )
    routes = route_ref[...]
    route_a, route_b = routes[0:1], routes[1:2]
    group_experts = expert_ref.shape[0] // groups
    group_at = lax.broadcasted_iota(jnp.int32, (groups, block), 0)
    inside = route_a - group_at * group_experts
    named = (inside >= 0) & (inside < group_experts)
    group_exp = jnp.exp(group_logits - jnp.max(group_logits, axis=0, keepdims=True))
    group_share = jnp.sum(jnp.where(named, group_exp, 0.0), axis=0, keepdims=True) / jnp.sum(
        group_exp, axis=0, keepdims=True
    )
    expert_at = lax.broadcasted_iota(jnp.int32, expert_logits.shape, 0)
    logit_a = jnp.sum(jnp.where(expert_at == route_a, expert_logits, 0.0), axis=0, keepdims=True)
    logit_b = jnp.sum(jnp.where(expert_at == route_b, expert_logits, 0.0), axis=0, keepdims=True)
    top = jnp.maximum(logit_a, logit_b)
    exp_a, exp_b = jnp.exp(logit_a - top), jnp.exp(logit_b - top)
    gate_a = group_share * (exp_a / (exp_a + exp_b))
    gate_b = group_share * (exp_b / (exp_a + exp_b))
    base = jnp.sum(jnp.where(named, group_at * group_experts, 0), axis=0, keepdims=True)
    lane_at = lax.broadcasted_iota(jnp.int32, (LANES // 2, block), 0)
    share_t = jnp.where(lane_at == route_a - base, gate_a, 0.0) + jnp.where(
        lane_at == route_b - base, gate_b, 0.0
    )
    coarse = share_t.astype(jnp.bfloat16)
    fine = (share_t - coarse.astype(jnp.float32)).astype(jnp.bfloat16)
    row_at = lax.broadcasted_iota(jnp.int32, (block, block), 0)
    column_at = lax.broadcasted_iota(jnp.int32, (block, block), 1)
    earlier = jnp.where(row_at < column_at, 1.0, 0.0).astype(jnp.bfloat16)
    counts = jnp.dot(
        jnp.where(named, 1.0, 0.0).astype(jnp.bfloat16), earlier, preferred_element_type=jnp.float32
    )
    first_row = (group_at * chunk).astype(jnp.float32)
    place = jnp.sum(jnp.where(named, counts + first_row, 0.0), axis=0, keepdims=True)
    take = jnp.where(row_at.astype(jnp.float32) == place, 1.0, 0.0).astype(jnp.bfloat16)
    xs_ref[:, :depth] = jnp.dot(take, normed, preferred_element_type=jnp.float32).astype(
        jnp.bfloat16
    )
    xs_ref[:, depth:] = lax.dot_general(
        take, jnp.concatenate([coarse, fine], axis=0), across, preferred_element_type=jnp.float32
    ).astype(jnp.bfloat16)
    with NS("barrier"):
        pl.semaphore_wait(barrier, len(peers))

    in_flight, used, names = {}, [0], {}

    def descriptor(source, target, device, sender, name):
        receiver = names.setdefault(name, len(names))
        return pltpu.make_async_remote_copy(
            src_ref=source,
            dst_ref=target,
            send_sem=send_sem.at[sender],
            recv_sem=recv_sem.at[receiver],
            device_id=device,
            device_id_type=MESH,
        )

    def send(name, source, target, device):
        sender = used[0] % send_sem.shape[0]
        used[0] += 1
        if sender in in_flight:
            in_flight[sender].wait_send()
        copy = descriptor(source, target, device, sender, name)
        copy.start()
        in_flight[sender] = copy

    def receive(name, target, scope=None):
        with NS(scope or "w" + name):
            descriptor(target, target, x_dev, 0, name).wait_recv()

    my_start = pl.multiple_of(group * chunk, chunk)
    units = UNITS(chunk)
    piece_rows = 16
    near_pair = pl.ds(mine + member * 2, 2)
    far_pair = pl.ds(mine + (1 - member) * 2, 2)
    width_half = depth // 2
    sides = (pl.ds(0, width_half), pl.ds(width_half, width_half))

    def span_of(u):
        return pl.ds(units[u][1], units[u][2])

    def own_rows(s, begin, count):
        if s == 0:
            return xs_ref.at[pl.ds(pl.multiple_of(my_start + begin, piece_rows), count)]
        return rows.at[s, own, pl.ds(begin, count)]

    def depart(u):
        s, begin, count = units[u]
        if s:
            there = pl.ds(pl.multiple_of(plane(s) * chunk + begin, piece_rows), count)
            send(f"z{u}", xs_ref.at[there], rows.at[s, own, span_of(u)], (plane(s) * 2 + member, tp))

    def arrive(u):
        s = units[u][0]
        receive(f"z{u}", rows.at[s, own, span_of(u)])

    def gather_x(u):
        s, begin, count = units[u]
        for i in range(count // piece_rows):
            at = begin + i * piece_rows
            target = rows.at[s, own, pl.ds(at, piece_rows)]
            send(f"x{u}{i}", own_rows(s, at, piece_rows), target, x_dev)

    def gather_y(u):
        s, begin, count = units[u]
        send(f"y{u}", own_rows(s, begin, count), rows.at[s, own, span_of(u)], y_dev)

    def relay(u, i):
        s, begin, count = units[u]
        block_at = rows.at[s, slot_x, pl.ds(begin + i * piece_rows, piece_rows)]
        receive(f"x{u}{i}", block_at)
        send(f"y{u}", block_at, block_at, y_dev)

    def core_near(u):
        s = units[u][0]
        pair = rows.at[s, near_pair, span_of(u)]
        send(f"core{u}", pair, pair, c_dev)

    def core_far(u):
        s = units[u][0]
        pair = rows.at[s, far_pair, span_of(u)]
        receive(f"y{u}", pair)
        send(f"core{u}", pair, pair, c_dev)

    def up(u, e):
        s, begin, count = units[u]
        if e == 0:
            receive(f"core{u}", rows.at[s, other_slots, span_of(u)])
        batch = 8 * count
        with NS(f"up{u}{e}"):
            tokens = rows[s, :, begin : begin + count, :depth].reshape(batch, depth)
            shares = rows[s, :, begin : begin + count, depth:].reshape(batch, LANES)
            lane = lax.broadcasted_iota(jnp.int32, shares.shape, 1) % (LANES // 2)
            wanted = lane == member * wg.shape[0] + e
            share = jnp.sum(
                jnp.where(wanted, shares.astype(jnp.float32), 0.0), axis=1, keepdims=True
            )
            pre = jnp.dot(tokens, wg[e], preferred_element_type=jnp.float32)
            high = jnp.dot(tokens, wu[e], preferred_element_type=jnp.float32)
            act[e, :batch] = (jax.nn.silu(pre) * high * share).astype(jnp.bfloat16)

    def down(u):
        s, begin, count = units[u]
        batch = 8 * count
        tile = 512
        acts = jnp.concatenate([act[e, :batch] for e in range(wg.shape[0])], axis=1)

        def column(n, carry):
            columns = pl.ds(pl.multiple_of(n * tile, tile), tile)
            value = jnp.dot(acts, wd[:, columns], preferred_element_type=jnp.float32)
            part[s, :, begin : begin + count, columns] = value.astype(jnp.bfloat16).reshape(
                8, count, tile
            )
            return carry

        with NS(f"down{u}"):
            for i, side in enumerate(sides):
                tiles = width_half // tile
                lax.fori_loop(i * tiles, (i + 1) * tiles, column, 0)
                send(
                    f"sum{u}",
                    part.at[s, other_slots, span_of(u), side],
                    from_core.at[s, :, span_of(u), side],
                    c_dev,
                )

    def experts(u):
        for e in range(wg.shape[0]):
            up(u, e)
        down(u)

    def add(index, term):
        part[index] = (part[index].astype(jnp.float32) + term.astype(jnp.float32)).astype(
            jnp.bfloat16
        )

    def scatter(u):
        s, begin, count = units[u]
        span = span_of(u)
        left, right = sides
        receive(f"sum{u}", from_core.at[s, :, span])
        with NS(f"E{u}"):
            add((s, mine_slots, span), from_core[s, :, span])
        send(f"dy{u}", part.at[s, slot_d, span, left], relay_y.at[s, span], y_dev)
        send(f"dx{u}", part.at[s, slot_d, span, right], relay_x.at[s, span], x_dev)
        send(f"xy{u}", part.at[s, slot_x, span, right], from_xy.at[s, 0, span, right], x_dev)
        send(f"xy{u}", part.at[s, slot_y, span, left], from_xy.at[s, 1, span, left], y_dev)

    def scatter_relay(u):
        s, begin, count = units[u]
        span = span_of(u)
        left, right = sides
        receive(f"dy{u}", relay_y.at[s, span])
        add((s, slot_x, span, left), relay_y[s, span])
        send(f"xy{u}", part.at[s, slot_x, span, left], from_xy.at[s, 0, span, left], x_dev)
        receive(f"dx{u}", relay_x.at[s, span])
        add((s, slot_y, span, right), relay_x[s, span])
        send(f"xy{u}", part.at[s, slot_y, span, right], from_xy.at[s, 1, span, right], y_dev)

    def home(u):
        s, begin, count = units[u]
        span = span_of(u)
        receive(f"xy{u}", from_xy.at[s, :, span], f"wH{u}")
        summed = (
            part[s, own, span].astype(jnp.float32)
            + from_xy[s, 0, span].astype(jnp.float32)
            + from_xy[s, 1, span].astype(jnp.float32)
        ).astype(jnp.bfloat16)
        there = pl.ds(pl.multiple_of(my_start + begin, piece_rows), count)
        if s:
            total[s, span] = summed
            to = (group + groups - s) % groups
            send(f"home{u}", total.at[s, span], back.at[there], (to * 2 + member, tp))
        else:
            back[there] = summed

    def settle(u):
        s, begin, count = units[u]
        if s:
            there = pl.ds(pl.multiple_of(plane(s) * chunk + begin, piece_rows), count)
            receive(f"home{u}", back.at[there])

    head_count = q_ref.shape[1] // HD
    query_at = lax.broadcasted_iota(jnp.int32, (WINDOW, 2 * WINDOW), 0)
    key_at = lax.broadcasted_iota(jnp.int32, (WINDOW, 2 * WINDOW), 1)
    distance = query_at + WINDOW - key_at
    near = (distance >= 0) & (distance < WINDOW)

    def attend(b, carry):
        start = pl.multiple_of(b * WINDOW, WINDOW)
        keys = k_ext[:, pl.ds(start, 2 * WINDOW)]
        band = v_ext[:, pl.ds(start, 2 * WINDOW)]
        queries = q_ref[pl.ds(start, WINDOW)]
        allowed = near & (key_at + (ep * row_count + b * WINDOW - WINDOW) >= 0)
        outs = []
        for h in range(head_count):
            query = queries[:, h * HD : (h + 1) * HD]
            scores = jnp.dot(query, keys, preferred_element_type=jnp.float32) * HD ** (-0.5)
            masked = jnp.where(allowed, scores, -1e30)
            sink = jnp.full((WINDOW, 1), sink_ref[h], jnp.float32)
            row_max = jnp.maximum(jnp.max(masked, axis=1, keepdims=True), sink)
            weights = jnp.exp(masked - row_max)
            denominator = jnp.sum(weights, axis=1, keepdims=True) + jnp.exp(sink - row_max)
            probs = (weights * (1.0 / denominator)).astype(jnp.bfloat16)
            outs.append(lax.dot_general(probs, band, across, preferred_element_type=jnp.float32))
        heads[tp, pl.ds(start, WINDOW)] = jnp.concatenate(outs, axis=1).astype(jnp.bfloat16)
        return carry

    def att(first_block, last_block):
        with NS(f"att{first_block}"):
            lax.fori_loop(first_block, last_block, attend, 0)

    blocks = row_count // WINDOW
    pieces = 4
    piece = row_count // pieces
    per = blocks // pieces

    def send_heads(i):
        span = pl.ds(i * piece, piece)
        send("heads_x", heads.at[tp, span], heads.at[tp, span], x_dev)

    def share_heads():
        send("heads_c", heads.at[tp], heads.at[tp], c_dev)

    def relay_heads():
        receive("heads_x", heads.at[tp_x])
        send("heads_cx", heads.at[tp_x], heads.at[tp_x], c_dev)

    def await_heads():
        receive("heads_c", heads.at[tp_c])
        receive("heads_cx", heads.at[tp_c])

    written = []

    def project(i):
        span = pl.ds(i * piece, piece)
        with NS(f"proj{i}"):
            joined = jnp.concatenate([heads[t, span] for t in range(4)], axis=1)
            mixed[span] = jnp.dot(joined, proj[...], preferred_element_type=jnp.float32).astype(
                jnp.bfloat16
            )
        copy = pltpu.make_async_copy(mixed.at[span], mixer_hbm.at[span], out_sem.at[1 + i])
        copy.start()
        written.append(copy)

    with NS("wqkv"):
        for load in middle:
            load.wait()
    for name, ext in (("k", k_ext), ("v", v_ext)):
        send(name, ext.at[:, pl.ds(row_count, WINDOW)], ext.at[:, pl.ds(0, WINDOW)], next_dev)
    gather_x(FIRST)
    gather_y(FIRST)
    depart("1")
    keep = pltpu.make_async_copy(
        xs_ref.at[pl.ds(my_start, chunk)], rows.at[0, own], out_sem.at[0]
    )
    keep.start()

    def take_halo():
        for name, ext in (("k", k_ext), ("v", v_ext)):
            receive(name, ext.at[:, pl.ds(0, WINDOW)])

    def take_weights():
        with NS("loads"):
            for load in late:
                load.wait()

    att(2, 4)
    send_heads(1)
    att(4, 6)
    depart("2")
    relay("0", 0)
    relay("0", 1)
    att(6, 7)
    arrive("1")
    gather_x("1")
    gather_y("1")
    att(7, 8)
    att(1, 2)
    take_halo()
    depart("a")
    depart("b")
    att(0, 1)
    share_heads()
    take_weights()
    keep.wait()
    core_near("0")
    arrive("2")
    gather_x("2")
    core_far("0")
    relay("1", 0)
    relay("1", 1)
    gather_y("2")
    core_near("1")
    arrive("a")
    gather_x("a")
    arrive("b")
    gather_x("b")
    up("0", 0)
    up("0", 1)
    relay("2", 0)
    send_heads(2)
    send_heads(3)
    send_heads(0)
    down("0")
    relay("2", 1)
    gather_y("a")
    core_near("2")
    core_far("1")
    relay("a", 0)
    gather_y("b")
    core_near("a")
    relay("b", 0)
    core_near("b")
    up("1", 0)
    up("1", 1)
    down("1")
    core_far("2")
    scatter("1")
    up("2", 0)
    up("2", 1)
    core_far("a")
    down("2")
    core_far("b")
    scatter("2")
    relay_heads()
    scatter_relay("1")
    experts("a")
    scatter_relay("2")
    experts("b")
    scatter("a")
    home("1")
    scatter("b")
    home("2")
    scatter_relay("a")
    scatter("0")
    await_heads()
    project(0)
    scatter_relay("b")
    home("a")
    project(1)
    scatter_relay("0")
    home("b")
    project(2)
    project(3)
    home("0")
    settle("1")
    settle("2")
    settle("a")
    settle("b")
    with NS("finish"):
        moved[...] = lax.dot_general(
            take, back[...], (((0,), (0,)), ((), ())), preferred_element_type=jnp.float32
        ).astype(jnp.bfloat16)
    copy = pltpu.make_async_copy(moved, out_hbm, out_sem.at[1 + pieces])
    copy.start()
    written.append(copy)
    with NS("wsend"):
        for copy in in_flight.values():
            copy.wait_send()
    with NS("wout"):
        for copy in written:
            copy.wait()


def fused(
    sinks,
    q_heads,
    k_heads,
    v_heads,
    gain,
    router_group,
    router_expert,
    routes,
    tokens_b,
    expert_gate,
    expert_up,
    expert_down,
    proj,
):
    groups = router_group.shape[1]
    block = tokens_b.shape[0] // 4
    experts, depth, hidden = expert_gate.shape
    width = depth + LANES
    row_count, head_width = q_heads.shape
    down = expert_down.reshape(experts * hidden, depth)
    chunk = block // groups
    bf16 = jnp.bfloat16
    anywhere = pl.BlockSpec(memory_space=pl.ANY)
    return pl.pallas_call(
        functools.partial(fused_kernel, groups),
        out_shape=(
            jax.ShapeDtypeStruct((row_count, proj.shape[1]), bf16),
            jax.ShapeDtypeStruct((block, depth), bf16),
        ),
        in_specs=[anywhere] * 13,
        out_specs=(anywhere, anywhere),
        scratch_shapes=[
            pltpu.SMEM(sinks.shape, jnp.float32),
            pltpu.VMEM(q_heads.shape, bf16),
            pltpu.VMEM((1, depth), jnp.float32),
            pltpu.VMEM((groups, depth), bf16),
            pltpu.VMEM((router_expert.shape[1], depth), bf16),
            pltpu.VMEM((2, block), jnp.int32),
            pltpu.VMEM((HD, row_count + WINDOW), bf16),
            pltpu.VMEM((HD, row_count + WINDOW), bf16),
            pltpu.VMEM((block, depth), bf16),
            pltpu.VMEM((block, width), bf16),
            pltpu.VMEM((4, row_count, head_width), bf16),
            pltpu.VMEM((groups, 8, chunk, width), bf16),
            pltpu.VMEM((groups, 8, chunk, depth), bf16),
            pltpu.VMEM(expert_gate.shape, bf16),
            pltpu.VMEM(expert_up.shape, bf16),
            pltpu.VMEM(down.shape, bf16),
            pltpu.VMEM(proj.shape, bf16),
            pltpu.VMEM((experts, 8 * chunk, hidden), bf16),
            pltpu.VMEM((groups, 4, chunk, depth), bf16),
            pltpu.VMEM((groups, chunk, depth // 2), bf16),
            pltpu.VMEM((groups, chunk, depth // 2), bf16),
            pltpu.VMEM((groups, 2, chunk, depth), bf16),
            pltpu.VMEM((groups, chunk, depth), bf16),
            pltpu.VMEM((block, depth), bf16),
            pltpu.VMEM((row_count, proj.shape[1]), bf16),
            pltpu.VMEM((block, depth), bf16),
            pltpu.SemaphoreType.DMA((13,)),
            pltpu.SemaphoreType.DMA((6,)),
            pltpu.SemaphoreType.DMA((SENDERS,)),
            pltpu.SemaphoreType.DMA((RECEIVERS,)),
        ],
        cost_estimate=pl.CostEstimate(
            flops=20_000_000_000, bytes_accessed=20_000_000, transcendentals=0
        ),
        compiler_params=pltpu.CompilerParams(
            collective_id=0, has_side_effects=True, vmem_limit_bytes=56 * 2**20
        ),
    )(
        sinks,
        q_heads,
        k_heads.T,
        v_heads.T,
        gain[None, :],
        router_group.T,
        router_expert.T,
        routes.T,
        tokens_b,
        expert_gate,
        expert_up,
        down,
        proj,
    )


def per_device(
    q_heads,
    k_heads,
    v_heads,
    sink_logits,
    out_weight,
    tokens_b,
    moe_gain,
    router_group,
    router_expert,
    route_expert,
    expert_gate,
    expert_up,
    expert_down,
):
    groups = router_group.shape[1]
    if (lax.axis_size("ep"), lax.axis_size("tp"), k_heads.shape[1]) == (2 * groups, 4, HD):
        return fused(
            sink_logits,
            q_heads,
            k_heads,
            v_heads,
            moe_gain,
            router_group,
            router_expert,
            route_expert,
            tokens_b,
            expert_gate,
            expert_up,
            expert_down,
            out_weight,
        )
    span_len = WINDOW
    row_count = q_heads.shape[0]
    kv_local = k_heads.shape[1] // HD
    group_size = HEADS // KV
    blocks = row_count // span_len
    stacked = jnp.stack([k_heads[row_count - span_len :], v_heads[row_count - span_len :]])
    earlier = shifted(stacked, "ep", 1)

    def make_band(own_rows, prev_rows):
        extended = jnp.concatenate([prev_rows, own_rows], axis=0).reshape(
            blocks + 1, span_len, kv_local, HD
        )
        return jnp.concatenate([extended[:-1], extended[1:]], axis=1)

    key_band = make_band(k_heads, earlier[0])
    value_band = make_band(v_heads, earlier[1])
    query_blocks = q_heads.reshape(blocks, span_len, kv_local, group_size, HD)
    scores = jnp.einsum(
        "nqhgd,nkhd->nhgqk", query_blocks, key_band, preferred_element_type=jnp.float32
    ) * HD ** (-0.5)
    first_row = lax.axis_index("ep") * row_count
    query_index = jnp.arange(span_len, dtype=jnp.int32)[:, None]
    key_index = jnp.arange(2 * span_len, dtype=jnp.int32)[None, :]
    distance = query_index + span_len - key_index
    key_place = (
        first_row
        + jnp.arange(blocks, dtype=jnp.int32)[:, None, None] * span_len
        + key_index[None]
        - span_len
    )
    allowed = (distance >= 0)[None] & (distance < span_len)[None] & (key_place >= 0)
    masked = jnp.where(allowed[:, None, None], scores, -1e30)
    sink_full = sink_logits.reshape(kv_local, group_size)[None, :, :, None]
    row_max = jnp.maximum(jnp.max(masked, axis=-1), sink_full)
    weights_exp = jnp.exp(masked - row_max[..., None])
    denominator = jnp.sum(weights_exp, axis=-1) + jnp.exp(sink_full - row_max)
    probs = (weights_exp / denominator[..., None]).astype(jnp.bfloat16)
    attended = jnp.einsum(
        "nhgqk,nkhd->nqhgd", probs, value_band, preferred_element_type=jnp.float32
    )
    attended = attended.astype(jnp.bfloat16).reshape(row_count, kv_local * group_size * HD)
    mixed = jnp.dot(
        lax.all_gather(attended, "tp", axis=1, tiled=True),
        out_weight,
        preferred_element_type=jnp.float32,
    )
    mixer_out = mixed.astype(jnp.bfloat16)
    tp_count = lax.axis_size("tp")
    tp_index = lax.axis_index("tp")
    exp_local = expert_gate.shape[0]
    expert_count = exp_local * lax.axis_size("ep")
    rows_dev = tokens_b.shape[0] // tp_count
    capacity = min(4 * rows_dev // expert_count, rows_dev // 4)
    own_routes = lax.dynamic_slice_in_dim(route_expert, tp_index * rows_dev, rows_dev, 0)
    own_normed = normalize(
        lax.dynamic_slice_in_dim(tokens_b, tp_index * rows_dev, rows_dev, 0), moe_gain
    )
    flat_routes, places = slot_positions(own_routes, 1, expert_count)
    buffer = fill_slots(own_normed, flat_routes, places, 1, expert_count, capacity, exp_local)
    delivered = lax.all_to_all(buffer, "ep", split_axis=0, concat_axis=0, tiled=True)
    arrived = lax.all_gather(delivered, "tp", axis=2, tiled=True)
    own_flat = flat_routes[0]
    own_places = places[0]
    gates = gate_weights(own_normed, own_routes, router_group, router_expert)
    gate_pre = jnp.einsum(
        "setcd,edf->setcf", arrived, expert_gate, preferred_element_type=jnp.float32
    )
    up_pre = jnp.einsum("setcd,edf->setcf", arrived, expert_up, preferred_element_type=jnp.float32)
    activated = (jax.nn.silu(gate_pre) * up_pre).astype(jnp.bfloat16)
    partial_value = jnp.einsum(
        "setcf,efd->setcd", activated, expert_down, preferred_element_type=jnp.float32
    )
    summed = lax.psum_scatter(
        partial_value.astype(jnp.bfloat16), "tp", scatter_dimension=2, tiled=True
    )
    returned = lax.all_to_all(summed, "ep", split_axis=0, concat_axis=0, tiled=True)
    returned = returned.reshape(expert_count * capacity, returned.shape[-1])
    picked_rows = returned[own_flat * capacity + own_places].reshape(
        rows_dev, 2, returned.shape[-1]
    )
    moe_out = jnp.sum(gates[:, :, None] * picked_rows.astype(jnp.float32), axis=1).astype(
        jnp.bfloat16
    )
    return (mixer_out, moe_out)


def solution(mesh):
    in_specs = (
        P("ep", "tp"),
        P("ep", "tp"),
        P("ep", "tp"),
        P("tp"),
        P(None, "tp"),
        P("ep", None),
        P(),
        P(),
        P(),
        P("ep", None),
        P("ep", None, "tp"),
        P("ep", None, "tp"),
        P("ep", "tp", None),
    )
    out_specs = (P("ep", "tp"), P(("ep", "tp"), None))
    return jax.shard_map(
        per_device, mesh=mesh, in_specs=in_specs, out_specs=out_specs, check_vma=False
    )
```

```python
import contextlib
import functools

import jax
import jax.numpy as jnp
from jax import lax
from jax.experimental import pallas as pl
from jax.experimental.pallas import tpu as pltpu
from jax.sharding import PartitionSpec as P

HEADS = 16
KV = 4
HD = 64
WINDOW = 128


def shifted(value, axis, steps):
    count = lax.axis_size(axis)
    leading, last = (max(0, -steps), min(count, count - steps))
    return lax.ppermute(value, axis, [(source, source + steps) for source in range(leading, last)])


def normalize(rows_in, gain):
    values = rows_in.astype(jnp.float32)
    scaled = values * lax.rsqrt(jnp.mean(values * values, axis=-1, keepdims=True) + 1e-06) * gain
    return scaled.astype(jnp.bfloat16)


def gate_weights(normed, routes, router_group, router_expert):
    group_logits = jnp.dot(normed, router_group, preferred_element_type=jnp.float32)
    expert_logits = jnp.dot(normed, router_expert, preferred_element_type=jnp.float32)
    group_count = router_group.shape[1]
    expert_count = router_expert.shape[1]
    chosen_group = routes[:, 0] // (expert_count // group_count)
    group_match = chosen_group[:, None] == jnp.arange(group_count, dtype=jnp.int32)[None, :]
    group_share = jnp.sum(
        jnp.where(group_match, jax.nn.softmax(group_logits, axis=-1), 0.0), axis=-1
    )
    expert_match = routes[:, :, None] == jnp.arange(expert_count, dtype=jnp.int32)[None, None, :]
    picked = jnp.sum(jnp.where(expert_match, expert_logits[:, None, :], 0.0), axis=-1)
    return group_share[:, None] * jax.nn.softmax(picked, axis=-1)


def slot_positions(routes, sub_count, expert_count):
    flat_routes = routes.reshape(sub_count, -1)
    onehot = (
        flat_routes[:, :, None] == jnp.arange(expert_count, dtype=jnp.int32)[None, None, :]
    ).astype(jnp.int32)
    places = jnp.sum(onehot * jnp.cumsum(onehot, axis=1), axis=2) - 1
    return (flat_routes, places)


def fill_slots(normed, flat_routes, places, sub_count, expert_count, capacity, exp_local):
    sub_index = jnp.arange(sub_count, dtype=jnp.int32)[:, None]
    target = ((flat_routes * sub_count + sub_index) * capacity + places).reshape(-1)
    source = jnp.repeat(normed, 2, axis=0)
    buffer = jnp.zeros((expert_count * sub_count * capacity, normed.shape[1]), jnp.bfloat16)
    buffer = buffer.at[target].set(source)
    return buffer.reshape(
        expert_count // exp_local, exp_local, sub_count, capacity, normed.shape[1]
    )


LANES = 128
MESH = pl.DeviceIdType.MESH


@contextlib.contextmanager
def NS(name):
    pl.delay(1)
    yield
    pl.delay(1)

FIRST = "0"
SENDERS = 24
RECEIVERS = 51


def UNITS(chunk):
    half = chunk // 2
    return {
        "0": (0, 0, chunk),
        "1": (1, 0, chunk),
        "2": (2, 0, chunk),
        "a": (3, 0, half),
        "b": (3, half, half),
    }


def fused_kernel(
    groups,
    sink_hbm,
    q_hbm,
    k_hbm,
    v_hbm,
    gain_hbm,
    group_hbm,
    expert_hbm,
    route_hbm,
    tokens_hbm,
    gate_hbm,
    up_hbm,
    down_hbm,
    proj_hbm,
    mixed,
    moved,
    sink_ref,
    q_ref,
    gain_ref,
    group_ref,
    expert_ref,
    route_ref,
    k_ext,
    v_ext,
    tokens,
    xs_ref,
    heads,
    rows,
    part,
    wg,
    wu,
    wd,
    proj,
    act,
    from_core,
    relay_x,
    relay_y,
    from_xy,
    total,
    back,
    load_sem,
    out_sem,
    send_sem,
    recv_sem,
):
    ep, tp = lax.axis_index("ep"), lax.axis_index("tp")
    group, member = ep // 2, ep % 2
    x, core = tp // 2, tp % 2
    tp_x, tp_c = (1 - x) * 2 + core, x * 2 + (1 - core)
    ep_y = group * 2 + (1 - member)
    ep_count = groups * 2
    x_dev, y_dev, c_dev = (ep, tp_x), (ep_y, tp), (ep, tp_c)
    next_dev = ((ep + 1) % ep_count, tp)
    prev_dev = ((ep + ep_count - 1) % ep_count, tp)
    depth = back.shape[1]
    block = xs_ref.shape[0]
    chunk = block // groups
    row_count = q_ref.shape[0]
    mine, other = core * 4, (1 - core) * 4
    own = mine + member * 2 + x
    slot_x = mine + member * 2 + (1 - x)
    slot_y = mine + (1 - member) * 2 + x
    slot_d = mine + (1 - member) * 2 + (1 - x)
    mine_slots, other_slots = pl.ds(mine, 4), pl.ds(other, 4)

    def plane(step):
        return (group + step) % groups

    barrier = pltpu.get_barrier_semaphore()
    ahead = [plane(step) * 2 + member for step in range(1, groups)]
    peers = [(there, tp) for there in ahead] + [x_dev, y_dev, c_dev, next_dev, prev_dev]
    for peer in peers:
        pl.semaphore_signal(barrier, inc=1, device_id=peer, device_id_type=MESH)

    first = pl.multiple_of(tp * block, block)
    inner = pl.ds(WINDOW, row_count)
    pairs = (
        (tokens_hbm.at[pl.ds(first, block)], tokens),
        (gain_hbm, gain_ref),
        (group_hbm, group_ref),
        (expert_hbm, expert_ref),
        (route_hbm.at[:, pl.ds(first, block)], route_ref),
        (k_hbm, k_ext.at[:, inner]),
        (v_hbm, v_ext.at[:, inner]),
        (q_hbm, q_ref),
        (sink_hbm, sink_ref),
        (gate_hbm, wg),
        (up_hbm, wu),
        (down_hbm, wd),
        (proj_hbm, proj),
    )
    loads = [
        pltpu.make_async_copy(source, held, load_sem.at[i])
        for i, (source, held) in enumerate(pairs)
    ]
    early, middle, late = loads[:5], loads[5:9], loads[9:]
    for load in early + middle:
        load.start()
    with NS("wearly"):
        for load in early:
            load.wait()
    for load in late:
        load.start()
    values = tokens[...].astype(jnp.float32)
    scale = lax.rsqrt(jnp.mean(values * values, axis=1, keepdims=True) + 1e-06)
    normed = (values * scale * gain_ref[...]).astype(jnp.bfloat16)
    across = (((1,), (1,)), ((), ()))
    group_logits = lax.dot_general(
        group_ref[...], normed, across, preferred_element_type=jnp.float32
    )
    expert_logits = lax.dot_general(
        expert_ref[...], normed, across, preferred_element_type=jnp.float32
    )
    routes = route_ref[...]
    route_a, route_b = routes[0:1], routes[1:2]
    group_experts = expert_ref.shape[0] // groups
    group_at = lax.broadcasted_iota(jnp.int32, (groups, block), 0)
    inside = route_a - group_at * group_experts
    named = (inside >= 0) & (inside < group_experts)
    group_exp = jnp.exp(group_logits - jnp.max(group_logits, axis=0, keepdims=True))
    group_share = jnp.sum(jnp.where(named, group_exp, 0.0), axis=0, keepdims=True) / jnp.sum(
        group_exp, axis=0, keepdims=True
    )
    expert_at = lax.broadcasted_iota(jnp.int32, expert_logits.shape, 0)
    logit_a = jnp.sum(jnp.where(expert_at == route_a, expert_logits, 0.0), axis=0, keepdims=True)
    logit_b = jnp.sum(jnp.where(expert_at == route_b, expert_logits, 0.0), axis=0, keepdims=True)
    top = jnp.maximum(logit_a, logit_b)
    exp_a, exp_b = jnp.exp(logit_a - top), jnp.exp(logit_b - top)
    gate_a = group_share * (exp_a / (exp_a + exp_b))
    gate_b = group_share * (exp_b / (exp_a + exp_b))
    base = jnp.sum(jnp.where(named, group_at * group_experts, 0), axis=0, keepdims=True)
    lane_at = lax.broadcasted_iota(jnp.int32, (LANES // 2, block), 0)
    share_t = jnp.where(lane_at == route_a - base, gate_a, 0.0) + jnp.where(
        lane_at == route_b - base, gate_b, 0.0
    )
    coarse = share_t.astype(jnp.bfloat16)
    fine = (share_t - coarse.astype(jnp.float32)).astype(jnp.bfloat16)
    row_at = lax.broadcasted_iota(jnp.int32, (block, block), 0)
    column_at = lax.broadcasted_iota(jnp.int32, (block, block), 1)
    earlier = jnp.where(row_at < column_at, 1.0, 0.0).astype(jnp.bfloat16)
    counts = jnp.dot(
        jnp.where(named, 1.0, 0.0).astype(jnp.bfloat16), earlier, preferred_element_type=jnp.float32
    )
    first_row = (group_at * chunk).astype(jnp.float32)
    place = jnp.sum(jnp.where(named, counts + first_row, 0.0), axis=0, keepdims=True)
    take = jnp.where(row_at.astype(jnp.float32) == place, 1.0, 0.0).astype(jnp.bfloat16)
    xs_ref[:, :depth] = jnp.dot(take, normed, preferred_element_type=jnp.float32).astype(
        jnp.bfloat16
    )
    xs_ref[:, depth:] = lax.dot_general(
        take, jnp.concatenate([coarse, fine], axis=0), across, preferred_element_type=jnp.float32
    ).astype(jnp.bfloat16)
    with NS("barrier"):
        pl.semaphore_wait(barrier, len(peers))

    in_flight, used, names = {}, [0], {}

    def descriptor(source, target, device, sender, name):
        receiver = names.setdefault(name, len(names))
        return pltpu.make_async_remote_copy(
            src_ref=source,
            dst_ref=target,
            send_sem=send_sem.at[sender],
            recv_sem=recv_sem.at[receiver],
            device_id=device,
            device_id_type=MESH,
        )

    def send(name, source, target, device):
        sender = used[0] % send_sem.shape[0]
        used[0] += 1
        if sender in in_flight:
            in_flight[sender].wait_send()
        copy = descriptor(source, target, device, sender, name)
        copy.start()
        in_flight[sender] = copy

    def receive(name, target, scope=None):
        with NS(scope or "w" + name):
            descriptor(target, target, x_dev, 0, name).wait_recv()

    my_start = pl.multiple_of(group * chunk, chunk)
    units = UNITS(chunk)
    piece_rows = 16
    near_pair = pl.ds(mine + member * 2, 2)
    far_pair = pl.ds(mine + (1 - member) * 2, 2)
    width_half = depth // 2
    sides = (pl.ds(0, width_half), pl.ds(width_half, width_half))

    def span_of(u):
        return pl.ds(units[u][1], units[u][2])

    def own_rows(s, begin, count):
        if s == 0:
            return xs_ref.at[pl.ds(pl.multiple_of(my_start + begin, piece_rows), count)]
        return rows.at[s, own, pl.ds(begin, count)]

    def depart(u):
        s, begin, count = units[u]
        if s:
            there = pl.ds(pl.multiple_of(plane(s) * chunk + begin, piece_rows), count)
            send(f"z{u}", xs_ref.at[there], rows.at[s, own, span_of(u)], (plane(s) * 2 + member, tp))

    def arrive(u):
        s = units[u][0]
        receive(f"z{u}", rows.at[s, own, span_of(u)])

    def gather_x(u):
        s, begin, count = units[u]
        for i in range(count // piece_rows):
            at = begin + i * piece_rows
            target = rows.at[s, own, pl.ds(at, piece_rows)]
            send(f"x{u}{i}", own_rows(s, at, piece_rows), target, x_dev)

    def gather_y(u):
        s, begin, count = units[u]
        send(f"y{u}", own_rows(s, begin, count), rows.at[s, own, span_of(u)], y_dev)

    def relay(u, i):
        s, begin, count = units[u]
        block_at = rows.at[s, slot_x, pl.ds(begin + i * piece_rows, piece_rows)]
        receive(f"x{u}{i}", block_at)
        send(f"y{u}", block_at, block_at, y_dev)

    def core_near(u):
        s = units[u][0]
        pair = rows.at[s, near_pair, span_of(u)]
        send(f"core{u}", pair, pair, c_dev)

    def core_far(u):
        s = units[u][0]
        pair = rows.at[s, far_pair, span_of(u)]
        receive(f"y{u}", pair)
        send(f"core{u}", pair, pair, c_dev)

    def up(u, e):
        s, begin, count = units[u]
        if e == 0:
            receive(f"core{u}", rows.at[s, other_slots, span_of(u)])
        batch = 8 * count
        with NS(f"up{u}{e}"):
            tokens = rows[s, :, begin : begin + count, :depth].reshape(batch, depth)
            shares = rows[s, :, begin : begin + count, depth:].reshape(batch, LANES)
            lane = lax.broadcasted_iota(jnp.int32, shares.shape, 1) % (LANES // 2)
            wanted = lane == member * wg.shape[0] + e
            share = jnp.sum(
                jnp.where(wanted, shares.astype(jnp.float32), 0.0), axis=1, keepdims=True
            )
            pre = jnp.dot(tokens, wg[e], preferred_element_type=jnp.float32)
            high = jnp.dot(tokens, wu[e], preferred_element_type=jnp.float32)
            act[e, :batch] = (jax.nn.silu(pre) * high * share).astype(jnp.bfloat16)

    def down(u):
        s, begin, count = units[u]
        batch = 8 * count
        tile = 512
        acts = jnp.concatenate([act[e, :batch] for e in range(wg.shape[0])], axis=1)

        def column(n, carry):
            columns = pl.ds(pl.multiple_of(n * tile, tile), tile)
            value = jnp.dot(acts, wd[:, columns], preferred_element_type=jnp.float32)
            part[s, :, begin : begin + count, columns] = value.astype(jnp.bfloat16).reshape(
                8, count, tile
            )
            return carry

        with NS(f"down{u}"):
            for i, side in enumerate(sides):
                tiles = width_half // tile
                lax.fori_loop(i * tiles, (i + 1) * tiles, column, 0)
                send(
                    f"sum{u}",
                    part.at[s, other_slots, span_of(u), side],
                    from_core.at[s, :, span_of(u), side],
                    c_dev,
                )

    def experts(u):
        for e in range(wg.shape[0]):
            up(u, e)
        down(u)

    def add(index, term):
        part[index] = (part[index].astype(jnp.float32) + term.astype(jnp.float32)).astype(
            jnp.bfloat16
        )

    def scatter(u):
        scatter_far(u)
        scatter_near(u)

    def scatter_far(u):
        s, begin, count = units[u]
        span = span_of(u)
        left, right = sides
        receive(f"sum{u}", from_core.at[s, :, span])
        with NS(f"E{u}"):
            add((s, mine_slots, span), from_core[s, :, span])
        send(f"dy{u}", part.at[s, slot_d, span, left], relay_y.at[s, span], y_dev)
        send(f"dx{u}", part.at[s, slot_d, span, right], relay_x.at[s, span], x_dev)

    def scatter_near(u):
        s, begin, count = units[u]
        span = span_of(u)
        left, right = sides
        send(f"xy{u}", part.at[s, slot_x, span, right], from_xy.at[s, 0, span, right], x_dev)
        send(f"xy{u}", part.at[s, slot_y, span, left], from_xy.at[s, 1, span, left], y_dev)

    def scatter_relay(u):
        s, begin, count = units[u]
        span = span_of(u)
        left, right = sides
        receive(f"dy{u}", relay_y.at[s, span])
        add((s, slot_x, span, left), relay_y[s, span])
        send(f"xy{u}", part.at[s, slot_x, span, left], from_xy.at[s, 0, span, left], x_dev)
        receive(f"dx{u}", relay_x.at[s, span])
        add((s, slot_y, span, right), relay_x[s, span])
        send(f"xy{u}", part.at[s, slot_y, span, right], from_xy.at[s, 1, span, right], y_dev)

    def home(u):
        s, begin, count = units[u]
        span = span_of(u)
        receive(f"xy{u}", from_xy.at[s, :, span], f"wH{u}")
        summed = (
            part[s, own, span].astype(jnp.float32)
            + from_xy[s, 0, span].astype(jnp.float32)
            + from_xy[s, 1, span].astype(jnp.float32)
        ).astype(jnp.bfloat16)
        there = pl.ds(pl.multiple_of(my_start + begin, piece_rows), count)
        if s:
            total[s, span] = summed
            to = (group + groups - s) % groups
            send(f"home{u}", total.at[s, span], back.at[there], (to * 2 + member, tp))
        else:
            back[there] = summed

    def settle(u):
        s, begin, count = units[u]
        if s:
            there = pl.ds(pl.multiple_of(plane(s) * chunk + begin, piece_rows), count)
            receive(f"home{u}", back.at[there])

    head_count = q_ref.shape[1] // HD
    query_at = lax.broadcasted_iota(jnp.int32, (WINDOW, 2 * WINDOW), 0)
    key_at = lax.broadcasted_iota(jnp.int32, (WINDOW, 2 * WINDOW), 1)
    distance = query_at + WINDOW - key_at
    near = (distance >= 0) & (distance < WINDOW)

    def attend(b, carry):
        start = pl.multiple_of(b * WINDOW, WINDOW)
        keys = k_ext[:, pl.ds(start, 2 * WINDOW)]
        band = v_ext[:, pl.ds(start, 2 * WINDOW)]
        queries = q_ref[pl.ds(start, WINDOW)]
        allowed = near & (key_at + (ep * row_count + b * WINDOW - WINDOW) >= 0)
        outs = []
        for h in range(head_count):
            query = queries[:, h * HD : (h + 1) * HD]
            scores = jnp.dot(query, keys, preferred_element_type=jnp.float32) * HD ** (-0.5)
            masked = jnp.where(allowed, scores, -1e30)
            sink = jnp.full((WINDOW, 1), sink_ref[h], jnp.float32)
            row_max = jnp.maximum(jnp.max(masked, axis=1, keepdims=True), sink)
            weights = jnp.exp(masked - row_max)
            denominator = jnp.sum(weights, axis=1, keepdims=True) + jnp.exp(sink - row_max)
            probs = (weights * (1.0 / denominator)).astype(jnp.bfloat16)
            outs.append(lax.dot_general(probs, band, across, preferred_element_type=jnp.float32))
        heads[tp, pl.ds(start, WINDOW)] = jnp.concatenate(outs, axis=1).astype(jnp.bfloat16)
        return carry

    def att(first_block, last_block):
        with NS(f"att{first_block}"):
            lax.fori_loop(first_block, last_block, attend, 0)

    blocks = row_count // WINDOW
    pieces = 4
    piece = row_count // pieces
    per = blocks // pieces

    def send_heads(i):
        span = pl.ds(i * piece, piece)
        send("heads_x", heads.at[tp, span], heads.at[tp, span], x_dev)

    def share_heads():
        send("heads_c", heads.at[tp], heads.at[tp], c_dev)

    def relay_heads():
        receive("heads_x", heads.at[tp_x])
        send("heads_cx", heads.at[tp_x], heads.at[tp_x], c_dev)

    def await_heads():
        receive("heads_c", heads.at[tp_c])
        receive("heads_cx", heads.at[tp_c])

    def project(i):
        span = pl.ds(i * piece, piece)
        with NS(f"proj{i}"):
            joined = jnp.concatenate([heads[t, span] for t in range(4)], axis=1)
            mixed[span] = jnp.dot(joined, proj[...], preferred_element_type=jnp.float32).astype(
                jnp.bfloat16
            )

    with NS("wqkv"):
        for load in middle:
            load.wait()
    for name, ext in (("k", k_ext), ("v", v_ext)):
        send(name, ext.at[:, pl.ds(row_count, WINDOW)], ext.at[:, pl.ds(0, WINDOW)], next_dev)
    gather_x(FIRST)
    gather_y(FIRST)
    depart("1")
    keep = pltpu.make_async_copy(
        xs_ref.at[pl.ds(my_start, chunk)], rows.at[0, own], out_sem.at[0]
    )
    keep.start()

    def take_halo():
        for name, ext in (("k", k_ext), ("v", v_ext)):
            receive(name, ext.at[:, pl.ds(0, WINDOW)])

    def take_weights():
        with NS("loads"):
            for load in late:
                load.wait()

    att(2, 4)
    send_heads(1)
    att(4, 6)
    depart("2")
    relay("0", 0)
    relay("0", 1)
    att(6, 7)
    arrive("1")
    gather_x("1")
    gather_y("1")
    att(7, 8)
    att(1, 2)
    take_halo()
    att(0, 1)
    share_heads()
    take_weights()
    keep.wait()
    core_near("0")
    core_far("0")
    relay("1", 0)
    relay("1", 1)
    depart("a")
    depart("b")
    core_near("1")
    arrive("2")
    gather_x("2")
    gather_y("2")
    send_heads(2)
    up("0", 0)
    up("0", 1)
    relay("2", 0)
    relay("2", 1)
    core_near("2")
    arrive("a")
    gather_x("a")
    gather_y("a")
    arrive("b")
    gather_x("b")
    gather_y("b")
    send_heads(3)
    send_heads(0)
    core_far("1")
    down("0")
    up("1", 0)
    relay("a", 0)
    core_near("a")
    up("1", 1)
    relay("b", 0)
    core_near("b")
    down("1")
    core_far("2")
    scatter("1")
    up("2", 0)
    up("2", 1)
    core_far("a")
    down("2")
    core_far("b")
    scatter_relay("1")
    scatter("2")
    relay_heads()
    experts("a")
    experts("b")
    scatter("a")
    scatter_relay("2")
    home("1")
    scatter("b")
    scatter_relay("a")
    scatter_far("0")
    await_heads()
    home("2")
    project(0)
    scatter_relay("b")
    scatter_near("0")
    home("a")
    project(1)
    scatter_relay("0")
    project(2)
    home("b")
    project(3)
    home("0")
    settle("1")
    settle("2")
    settle("a")
    settle("b")
    with NS("finish"):
        moved[...] = lax.dot_general(
            take, back[...], (((0,), (0,)), ((), ())), preferred_element_type=jnp.float32
        ).astype(jnp.bfloat16)
    with NS("wsend"):
        for copy in in_flight.values():
            copy.wait_send()


def store_kernel(mixed, moved, mixer_hbm, out_hbm, sem):
    copies = [
        pltpu.make_async_copy(source, target, sem.at[i])
        for i, (source, target) in enumerate(((mixed, mixer_hbm), (moved, out_hbm)))
    ]
    for copy in copies:
        copy.start()
    for copy in copies:
        copy.wait()


def store(mixed, moved):
    anywhere = pl.BlockSpec(memory_space=pl.ANY)
    return pl.pallas_call(
        store_kernel,
        out_shape=tuple(jax.ShapeDtypeStruct(v.shape, v.dtype) for v in (mixed, moved)),
        in_specs=[anywhere] * 2,
        out_specs=(anywhere, anywhere),
        scratch_shapes=[pltpu.SemaphoreType.DMA((2,))],
        compiler_params=pltpu.CompilerParams(vmem_limit_bytes=2**20),
    )(*(pltpu.with_memory_space_constraint(v, pltpu.VMEM) for v in (mixed, moved)))


def fused(
    sinks,
    q_heads,
    k_heads,
    v_heads,
    gain,
    router_group,
    router_expert,
    routes,
    tokens_b,
    expert_gate,
    expert_up,
    expert_down,
    proj,
):
    groups = router_group.shape[1]
    block = tokens_b.shape[0] // 4
    experts, depth, hidden = expert_gate.shape
    width = depth + LANES
    row_count, head_width = q_heads.shape
    down = expert_down.reshape(experts * hidden, depth)
    chunk = block // groups
    bf16 = jnp.bfloat16
    anywhere = pl.BlockSpec(memory_space=pl.ANY)
    mixed, moved = pl.pallas_call(
        functools.partial(fused_kernel, groups),
        out_shape=(
            pltpu.VMEM((row_count, proj.shape[1]), bf16),
            pltpu.VMEM((block, depth), bf16),
        ),
        in_specs=[anywhere] * 13,
        out_specs=(pl.BlockSpec(memory_space=pltpu.VMEM),) * 2,
        scratch_shapes=[
            pltpu.SMEM(sinks.shape, jnp.float32),
            pltpu.VMEM(q_heads.shape, bf16),
            pltpu.VMEM((1, depth), jnp.float32),
            pltpu.VMEM((groups, depth), bf16),
            pltpu.VMEM((router_expert.shape[1], depth), bf16),
            pltpu.VMEM((2, block), jnp.int32),
            pltpu.VMEM((HD, row_count + WINDOW), bf16),
            pltpu.VMEM((HD, row_count + WINDOW), bf16),
            pltpu.VMEM((block, depth), bf16),
            pltpu.VMEM((block, width), bf16),
            pltpu.VMEM((4, row_count, head_width), bf16),
            pltpu.VMEM((groups, 8, chunk, width), bf16),
            pltpu.VMEM((groups, 8, chunk, depth), bf16),
            pltpu.VMEM(expert_gate.shape, bf16),
            pltpu.VMEM(expert_up.shape, bf16),
            pltpu.VMEM(down.shape, bf16),
            pltpu.VMEM(proj.shape, bf16),
            pltpu.VMEM((experts, 8 * chunk, hidden), bf16),
            pltpu.VMEM((groups, 4, chunk, depth), bf16),
            pltpu.VMEM((groups, chunk, depth // 2), bf16),
            pltpu.VMEM((groups, chunk, depth // 2), bf16),
            pltpu.VMEM((groups, 2, chunk, depth), bf16),
            pltpu.VMEM((groups, chunk, depth), bf16),
            pltpu.VMEM((block, depth), bf16),
            pltpu.SemaphoreType.DMA((13,)),
            pltpu.SemaphoreType.DMA((1,)),
            pltpu.SemaphoreType.DMA((SENDERS,)),
            pltpu.SemaphoreType.DMA((RECEIVERS,)),
        ],
        cost_estimate=pl.CostEstimate(
            flops=20_000_000_000, bytes_accessed=20_000_000, transcendentals=0
        ),
        compiler_params=pltpu.CompilerParams(
            collective_id=0, has_side_effects=True, vmem_limit_bytes=40 * 2**20
        ),
    )(
        *(
            pltpu.with_memory_space_constraint(value, pltpu.HBM)
            for value in (
                sinks,
                q_heads,
                k_heads.T,
                v_heads.T,
                gain[None, :],
                router_group.T,
                router_expert.T,
                routes.T,
                tokens_b,
                expert_gate,
                expert_up,
                down,
                proj,
            )
        )
    )
    return store(mixed, moved)


def per_device(
    q_heads,
    k_heads,
    v_heads,
    sink_logits,
    out_weight,
    tokens_b,
    moe_gain,
    router_group,
    router_expert,
    route_expert,
    expert_gate,
    expert_up,
    expert_down,
):
    groups = router_group.shape[1]
    if (lax.axis_size("ep"), lax.axis_size("tp"), k_heads.shape[1]) == (2 * groups, 4, HD):
        return fused(
            sink_logits,
            q_heads,
            k_heads,
            v_heads,
            moe_gain,
            router_group,
            router_expert,
            route_expert,
            tokens_b,
            expert_gate,
            expert_up,
            expert_down,
            out_weight,
        )
    span_len = WINDOW
    row_count = q_heads.shape[0]
    kv_local = k_heads.shape[1] // HD
    group_size = HEADS // KV
    blocks = row_count // span_len
    stacked = jnp.stack([k_heads[row_count - span_len :], v_heads[row_count - span_len :]])
    earlier = shifted(stacked, "ep", 1)

    def make_band(own_rows, prev_rows):
        extended = jnp.concatenate([prev_rows, own_rows], axis=0).reshape(
            blocks + 1, span_len, kv_local, HD
        )
        return jnp.concatenate([extended[:-1], extended[1:]], axis=1)

    key_band = make_band(k_heads, earlier[0])
    value_band = make_band(v_heads, earlier[1])
    query_blocks = q_heads.reshape(blocks, span_len, kv_local, group_size, HD)
    scores = jnp.einsum(
        "nqhgd,nkhd->nhgqk", query_blocks, key_band, preferred_element_type=jnp.float32
    ) * HD ** (-0.5)
    first_row = lax.axis_index("ep") * row_count
    query_index = jnp.arange(span_len, dtype=jnp.int32)[:, None]
    key_index = jnp.arange(2 * span_len, dtype=jnp.int32)[None, :]
    distance = query_index + span_len - key_index
    key_place = (
        first_row
        + jnp.arange(blocks, dtype=jnp.int32)[:, None, None] * span_len
        + key_index[None]
        - span_len
    )
    allowed = (distance >= 0)[None] & (distance < span_len)[None] & (key_place >= 0)
    masked = jnp.where(allowed[:, None, None], scores, -1e30)
    sink_full = sink_logits.reshape(kv_local, group_size)[None, :, :, None]
    row_max = jnp.maximum(jnp.max(masked, axis=-1), sink_full)
    weights_exp = jnp.exp(masked - row_max[..., None])
    denominator = jnp.sum(weights_exp, axis=-1) + jnp.exp(sink_full - row_max)
    probs = (weights_exp / denominator[..., None]).astype(jnp.bfloat16)
    attended = jnp.einsum(
        "nhgqk,nkhd->nqhgd", probs, value_band, preferred_element_type=jnp.float32
    )
    attended = attended.astype(jnp.bfloat16).reshape(row_count, kv_local * group_size * HD)
    mixed = jnp.dot(
        lax.all_gather(attended, "tp", axis=1, tiled=True),
        out_weight,
        preferred_element_type=jnp.float32,
    )
    mixer_out = mixed.astype(jnp.bfloat16)
    tp_count = lax.axis_size("tp")
    tp_index = lax.axis_index("tp")
    exp_local = expert_gate.shape[0]
    expert_count = exp_local * lax.axis_size("ep")
    rows_dev = tokens_b.shape[0] // tp_count
    capacity = min(4 * rows_dev // expert_count, rows_dev // 4)
    own_routes = lax.dynamic_slice_in_dim(route_expert, tp_index * rows_dev, rows_dev, 0)
    own_normed = normalize(
        lax.dynamic_slice_in_dim(tokens_b, tp_index * rows_dev, rows_dev, 0), moe_gain
    )
    flat_routes, places = slot_positions(own_routes, 1, expert_count)
    buffer = fill_slots(own_normed, flat_routes, places, 1, expert_count, capacity, exp_local)
    delivered = lax.all_to_all(buffer, "ep", split_axis=0, concat_axis=0, tiled=True)
    arrived = lax.all_gather(delivered, "tp", axis=2, tiled=True)
    own_flat = flat_routes[0]
    own_places = places[0]
    gates = gate_weights(own_normed, own_routes, router_group, router_expert)
    gate_pre = jnp.einsum(
        "setcd,edf->setcf", arrived, expert_gate, preferred_element_type=jnp.float32
    )
    up_pre = jnp.einsum("setcd,edf->setcf", arrived, expert_up, preferred_element_type=jnp.float32)
    activated = (jax.nn.silu(gate_pre) * up_pre).astype(jnp.bfloat16)
    partial_value = jnp.einsum(
        "setcf,efd->setcd", activated, expert_down, preferred_element_type=jnp.float32
    )
    summed = lax.psum_scatter(
        partial_value.astype(jnp.bfloat16), "tp", scatter_dimension=2, tiled=True
    )
    returned = lax.all_to_all(summed, "ep", split_axis=0, concat_axis=0, tiled=True)
    returned = returned.reshape(expert_count * capacity, returned.shape[-1])
    picked_rows = returned[own_flat * capacity + own_places].reshape(
        rows_dev, 2, returned.shape[-1]
    )
    moe_out = jnp.sum(gates[:, :, None] * picked_rows.astype(jnp.float32), axis=1).astype(
        jnp.bfloat16
    )
    return (mixer_out, moe_out)


def solution(mesh):
    in_specs = (
        P("ep", "tp"),
        P("ep", "tp"),
        P("ep", "tp"),
        P("tp"),
        P(None, "tp"),
        P("ep", None),
        P(),
        P(),
        P(),
        P("ep", None),
        P("ep", None, "tp"),
        P("ep", None, "tp"),
        P("ep", "tp", None),
    )
    out_specs = (P("ep", "tp"), P(("ep", "tp"), None))
    return jax.shard_map(
        per_device, mesh=mesh, in_specs=in_specs, out_specs=out_specs, check_vma=False
    )
```

```python
import contextlib
import functools

import jax
import jax.numpy as jnp
from jax import lax
from jax.experimental import pallas as pl
from jax.experimental.pallas import tpu as pltpu
from jax.sharding import PartitionSpec as P

HEADS = 16
KV = 4
HD = 64
WINDOW = 128


def shifted(value, axis, steps):
    count = lax.axis_size(axis)
    leading, last = (max(0, -steps), min(count, count - steps))
    return lax.ppermute(value, axis, [(source, source + steps) for source in range(leading, last)])


def normalize(rows_in, gain):
    values = rows_in.astype(jnp.float32)
    scaled = values * lax.rsqrt(jnp.mean(values * values, axis=-1, keepdims=True) + 1e-06) * gain
    return scaled.astype(jnp.bfloat16)


def gate_weights(normed, routes, router_group, router_expert):
    group_logits = jnp.dot(normed, router_group, preferred_element_type=jnp.float32)
    expert_logits = jnp.dot(normed, router_expert, preferred_element_type=jnp.float32)
    group_count = router_group.shape[1]
    expert_count = router_expert.shape[1]
    chosen_group = routes[:, 0] // (expert_count // group_count)
    group_match = chosen_group[:, None] == jnp.arange(group_count, dtype=jnp.int32)[None, :]
    group_share = jnp.sum(
        jnp.where(group_match, jax.nn.softmax(group_logits, axis=-1), 0.0), axis=-1
    )
    expert_match = routes[:, :, None] == jnp.arange(expert_count, dtype=jnp.int32)[None, None, :]
    picked = jnp.sum(jnp.where(expert_match, expert_logits[:, None, :], 0.0), axis=-1)
    return group_share[:, None] * jax.nn.softmax(picked, axis=-1)


def slot_positions(routes, sub_count, expert_count):
    flat_routes = routes.reshape(sub_count, -1)
    onehot = (
        flat_routes[:, :, None] == jnp.arange(expert_count, dtype=jnp.int32)[None, None, :]
    ).astype(jnp.int32)
    places = jnp.sum(onehot * jnp.cumsum(onehot, axis=1), axis=2) - 1
    return (flat_routes, places)


def fill_slots(normed, flat_routes, places, sub_count, expert_count, capacity, exp_local):
    sub_index = jnp.arange(sub_count, dtype=jnp.int32)[:, None]
    target = ((flat_routes * sub_count + sub_index) * capacity + places).reshape(-1)
    source = jnp.repeat(normed, 2, axis=0)
    buffer = jnp.zeros((expert_count * sub_count * capacity, normed.shape[1]), jnp.bfloat16)
    buffer = buffer.at[target].set(source)
    return buffer.reshape(
        expert_count // exp_local, exp_local, sub_count, capacity, normed.shape[1]
    )


LANES = 128
MESH = pl.DeviceIdType.MESH


@contextlib.contextmanager
def NS(name):
    pl.delay(1)
    yield
    pl.delay(1)

FIRST = "0"
SENDERS = 24
RECEIVERS = 58


def UNITS(chunk):
    half = chunk // 2
    return {
        "0": (0, 0, chunk),
        "1": (1, 0, chunk),
        "c": (2, 0, half),
        "d": (2, half, half),
        "a": (3, 0, half),
        "b": (3, half, half),
    }


def fused_kernel(
    groups,
    sink_hbm,
    q_hbm,
    k_hbm,
    v_hbm,
    gain_hbm,
    group_hbm,
    expert_hbm,
    route_hbm,
    tokens_hbm,
    gate_hbm,
    up_hbm,
    down_hbm,
    proj_hbm,
    mixed,
    back,
    take_out,
    sink_ref,
    q_ref,
    gain_ref,
    group_ref,
    expert_ref,
    route_ref,
    k_ext,
    v_ext,
    tokens,
    xs_ref,
    share_ref,
    heads,
    rows,
    part,
    wg,
    wu,
    wd,
    proj,
    act,
    from_core,
    relay_x,
    relay_y,
    from_xy,
    total,
    load_sem,
    out_sem,
    send_sem,
    recv_sem,
):
    ep, tp = lax.axis_index("ep"), lax.axis_index("tp")
    group, member = ep // 2, ep % 2
    x, core = tp // 2, tp % 2
    tp_x, tp_c = (1 - x) * 2 + core, x * 2 + (1 - core)
    ep_y = group * 2 + (1 - member)
    ep_count = groups * 2
    x_dev, y_dev, c_dev, d_dev = (ep, tp_x), (ep_y, tp), (ep, tp_c), (ep_y, tp_x)
    next_dev = ((ep + 1) % ep_count, tp)
    prev_dev = ((ep + ep_count - 1) % ep_count, tp)
    depth = back.shape[1]
    block = xs_ref.shape[0]
    chunk = block // groups
    row_count = q_ref.shape[0]
    mine, other = core * 4, (1 - core) * 4
    own = mine + member * 2 + x
    slot_x = mine + member * 2 + (1 - x)
    slot_y = mine + (1 - member) * 2 + x
    slot_d = mine + (1 - member) * 2 + (1 - x)
    mine_slots, other_slots = pl.ds(mine, 4), pl.ds(other, 4)

    def plane(step):
        return (group + step) % groups

    barrier = pltpu.get_barrier_semaphore()
    ahead = [plane(step) * 2 + member for step in range(1, groups)]
    peers = [(there, tp) for there in ahead] + [x_dev, y_dev, c_dev, d_dev, next_dev, prev_dev]
    for peer in peers:
        pl.semaphore_signal(barrier, inc=1, device_id=peer, device_id_type=MESH)

    first = pl.multiple_of(tp * block, block)
    inner = pl.ds(WINDOW, row_count)
    pairs = (
        (tokens_hbm.at[pl.ds(first, block)], tokens),
        (gain_hbm, gain_ref),
        (group_hbm, group_ref),
        (expert_hbm, expert_ref),
        (route_hbm.at[:, pl.ds(first, block)], route_ref),
        (k_hbm, k_ext.at[:, inner]),
        (v_hbm, v_ext.at[:, inner]),
        (q_hbm, q_ref),
        (sink_hbm, sink_ref),
        (gate_hbm, wg),
        (up_hbm, wu),
        (down_hbm, wd),
        (proj_hbm, proj),
    )
    loads = [
        pltpu.make_async_copy(source, held, load_sem.at[i])
        for i, (source, held) in enumerate(pairs)
    ]
    early, middle, late = loads[:5], loads[5:9], loads[9:]
    for load in early + middle:
        load.start()
    early[4].wait()
    routes = route_ref[...]
    route_a, route_b = routes[0:1], routes[1:2]
    group_experts = expert_ref.shape[0] // groups
    group_at = lax.broadcasted_iota(jnp.int32, (groups, block), 0)
    inside = route_a - group_at * group_experts
    named = (inside >= 0) & (inside < group_experts)
    row_at = lax.broadcasted_iota(jnp.int32, (block, block), 0)
    column_at = lax.broadcasted_iota(jnp.int32, (block, block), 1)
    earlier = jnp.where(row_at < column_at, 1.0, 0.0).astype(jnp.bfloat16)
    counts = jnp.dot(
        jnp.where(named, 1.0, 0.0).astype(jnp.bfloat16), earlier, preferred_element_type=jnp.float32
    )
    first_row = (group_at * chunk).astype(jnp.float32)
    place = jnp.sum(jnp.where(named, counts + first_row, 0.0), axis=0, keepdims=True)
    take = jnp.where(row_at.astype(jnp.float32) == place, 1.0, 0.0).astype(jnp.bfloat16)
    with NS("wearly"):
        for load in early[:4]:
            load.wait()
    for load in late:
        load.start()
    values = tokens[...].astype(jnp.float32)
    scale = lax.rsqrt(jnp.mean(values * values, axis=1, keepdims=True) + 1e-06)
    normed = (values * scale * gain_ref[...]).astype(jnp.bfloat16)
    across = (((1,), (1,)), ((), ()))
    xs_ref[...] = jnp.dot(take, normed, preferred_element_type=jnp.float32).astype(jnp.bfloat16)
    take_out[...] = take
    with NS("barrier"):
        pl.semaphore_wait(barrier, len(peers))

    in_flight, used, names = {}, [0], {}

    def descriptor(source, target, device, sender, name):
        receiver = names.setdefault(name, len(names))
        return pltpu.make_async_remote_copy(
            src_ref=source,
            dst_ref=target,
            send_sem=send_sem.at[sender],
            recv_sem=recv_sem.at[receiver],
            device_id=device,
            device_id_type=MESH,
        )

    def send(name, source, target, device):
        sender = used[0] % send_sem.shape[0]
        used[0] += 1
        if sender in in_flight:
            in_flight[sender].wait_send()
        copy = descriptor(source, target, device, sender, name)
        copy.start()
        in_flight[sender] = copy

    def receive(name, target, scope=None):
        with NS(scope or "w" + name):
            descriptor(target, target, x_dev, 0, name).wait_recv()

    my_start = pl.multiple_of(group * chunk, chunk)
    units = UNITS(chunk)
    piece_rows = 16
    near_pair = pl.ds(mine + member * 2, 2)
    far_pair = pl.ds(mine + (1 - member) * 2, 2)
    width_half = depth // 2
    sides = (pl.ds(0, width_half), pl.ds(width_half, width_half))

    def span_of(u):
        return pl.ds(units[u][1], units[u][2])

    def own_rows(s, begin, count):
        if s == 0:
            return xs_ref.at[pl.ds(pl.multiple_of(my_start + begin, piece_rows), count)]
        return rows.at[s, own, pl.ds(begin, count)]

    def depart(u):
        s, begin, count = units[u]
        if s:
            there = pl.ds(pl.multiple_of(plane(s) * chunk + begin, piece_rows), count)
            send(f"z{u}", xs_ref.at[there], rows.at[s, own, span_of(u)], (plane(s) * 2 + member, tp))

    def arrive(u):
        s = units[u][0]
        receive(f"z{u}", rows.at[s, own, span_of(u)])

    def gather_x(u):
        s, begin, count = units[u]
        for i in range(count // piece_rows):
            at = begin + i * piece_rows
            target = rows.at[s, own, pl.ds(at, piece_rows)]
            send(f"x{u}{i}", own_rows(s, at, piece_rows), target, x_dev)

    def gather_y(u):
        s, begin, count = units[u]
        send(f"y{u}", own_rows(s, begin, count), rows.at[s, own, span_of(u)], y_dev)

    def relay(u, i):
        s, begin, count = units[u]
        block_at = rows.at[s, slot_x, pl.ds(begin + i * piece_rows, piece_rows)]
        receive(f"x{u}{i}", block_at)
        send(f"y{u}", block_at, block_at, y_dev)

    def core_near(u):
        s = units[u][0]
        pair = rows.at[s, near_pair, span_of(u)]
        send(f"core{u}", pair, pair, c_dev)

    def core_far(u):
        s = units[u][0]
        pair = rows.at[s, far_pair, span_of(u)]
        receive(f"y{u}", pair)
        send(f"core{u}", pair, pair, c_dev)

    def up(u, e):
        s, begin, count = units[u]
        if e == 0:
            receive(f"core{u}", rows.at[s, other_slots, span_of(u)])
        batch = 8 * count
        with NS(f"up{u}{e}"):
            tokens = rows[s, :, begin : begin + count].reshape(batch, depth)
            held = share_ref[s].astype(jnp.float32)
            at = lax.broadcasted_iota(jnp.int32, held.shape, 1) % group_experts
            wanted = at == member * wg.shape[0] + e
            by_lane = jnp.sum(jnp.where(wanted, held, 0.0), axis=1, keepdims=True)
            shape = (8, count, block)
            lane = lax.broadcasted_iota(jnp.int32, shape, 2) - group * chunk - begin
            picked = lane == lax.broadcasted_iota(jnp.int32, shape, 1)
            share = jnp.sum(
                jnp.where(picked, jnp.broadcast_to(by_lane, shape), 0.0), axis=2, keepdims=True
            ).reshape(batch, 1)
            pre = jnp.dot(tokens, wg[e], preferred_element_type=jnp.float32)
            high = jnp.dot(tokens, wu[e], preferred_element_type=jnp.float32)
            act[e, :batch] = (jax.nn.silu(pre) * high * share).astype(jnp.bfloat16)

    def down(u):
        s, begin, count = units[u]
        batch = 8 * count
        tile = 512
        acts = jnp.concatenate([act[e, :batch] for e in range(wg.shape[0])], axis=1)

        def column(n, carry):
            columns = pl.ds(pl.multiple_of(n * tile, tile), tile)
            value = jnp.dot(acts, wd[:, columns], preferred_element_type=jnp.float32)
            part[s, :, begin : begin + count, columns] = value.astype(jnp.bfloat16).reshape(
                8, count, tile
            )
            return carry

        with NS(f"down{u}"):
            for i, side in enumerate(sides):
                tiles = width_half // tile
                lax.fori_loop(i * tiles, (i + 1) * tiles, column, 0)
                send(
                    f"sum{u}",
                    part.at[s, other_slots, span_of(u), side],
                    from_core.at[s, :, span_of(u), side],
                    c_dev,
                )

    def experts(u):
        for e in range(wg.shape[0]):
            up(u, e)
        down(u)

    def add(index, term):
        part[index] = (part[index].astype(jnp.float32) + term.astype(jnp.float32)).astype(
            jnp.bfloat16
        )

    def scatter(u):
        scatter_far(u)
        scatter_near(u)

    def scatter_far(u):
        s, begin, count = units[u]
        span = span_of(u)
        left, right = sides
        receive(f"sum{u}", from_core.at[s, :, span])
        with NS(f"E{u}"):
            add((s, mine_slots, span), from_core[s, :, span])
        send(f"dy{u}", part.at[s, slot_d, span, left], relay_y.at[s, span], y_dev)
        send(f"dx{u}", part.at[s, slot_d, span, right], relay_x.at[s, span], x_dev)

    def scatter_near(u):
        s, begin, count = units[u]
        span = span_of(u)
        left, right = sides
        send(f"xy{u}", part.at[s, slot_x, span, right], from_xy.at[s, 0, span, right], x_dev)
        send(f"xy{u}", part.at[s, slot_y, span, left], from_xy.at[s, 1, span, left], y_dev)

    def scatter_relay(u):
        s, begin, count = units[u]
        span = span_of(u)
        left, right = sides
        receive(f"dy{u}", relay_y.at[s, span])
        add((s, slot_x, span, left), relay_y[s, span])
        send(f"xy{u}", part.at[s, slot_x, span, left], from_xy.at[s, 0, span, left], x_dev)
        receive(f"dx{u}", relay_x.at[s, span])
        add((s, slot_y, span, right), relay_x[s, span])
        send(f"xy{u}", part.at[s, slot_y, span, right], from_xy.at[s, 1, span, right], y_dev)

    def home(u):
        s, begin, count = units[u]
        span = span_of(u)
        receive(f"xy{u}", from_xy.at[s, :, span], f"wH{u}")
        summed = (
            part[s, own, span].astype(jnp.float32)
            + from_xy[s, 0, span].astype(jnp.float32)
            + from_xy[s, 1, span].astype(jnp.float32)
        ).astype(jnp.bfloat16)
        there = pl.ds(pl.multiple_of(my_start + begin, piece_rows), count)
        if s:
            total[s, span] = summed
            to = (group + groups - s) % groups
            send("home", total.at[s, span], back.at[there], (to * 2 + member, tp))
        else:
            back[there] = summed

    def settle():
        receive("home", back.at[pl.ds(0, block - chunk)])

    head_count = q_ref.shape[1] // HD
    query_at = lax.broadcasted_iota(jnp.int32, (WINDOW, 2 * WINDOW), 0)
    key_at = lax.broadcasted_iota(jnp.int32, (WINDOW, 2 * WINDOW), 1)
    distance = query_at + WINDOW - key_at
    near = (distance >= 0) & (distance < WINDOW)

    def attend(b, carry):
        start = pl.multiple_of(b * WINDOW, WINDOW)
        keys = k_ext[:, pl.ds(start, 2 * WINDOW)]
        band = v_ext[:, pl.ds(start, 2 * WINDOW)]
        queries = q_ref[pl.ds(start, WINDOW)]
        allowed = near & (key_at + (ep * row_count + b * WINDOW - WINDOW) >= 0)
        outs = []
        for h in range(head_count):
            query = queries[:, h * HD : (h + 1) * HD]
            scores = jnp.dot(query, keys, preferred_element_type=jnp.float32) * HD ** (-0.5)
            masked = jnp.where(allowed, scores, -1e30)
            sink = jnp.full((WINDOW, 1), sink_ref[h], jnp.float32)
            row_max = jnp.maximum(jnp.max(masked, axis=1, keepdims=True), sink)
            weights = jnp.exp(masked - row_max)
            denominator = jnp.sum(weights, axis=1, keepdims=True) + jnp.exp(sink - row_max)
            probs = (weights * (1.0 / denominator)).astype(jnp.bfloat16)
            outs.append(lax.dot_general(probs, band, across, preferred_element_type=jnp.float32))
        heads[tp, pl.ds(start, WINDOW)] = jnp.concatenate(outs, axis=1).astype(jnp.bfloat16)
        return carry

    def att(first_block, last_block):
        with NS(f"att{first_block}"):
            lax.fori_loop(first_block, last_block, attend, 0)

    blocks = row_count // WINDOW
    pieces = 4
    piece = row_count // pieces

    def send_heads(begin, end):
        span = pl.ds(begin * WINDOW, (end - begin) * WINDOW)
        send("heads_x", heads.at[tp, span], heads.at[tp, span], x_dev)

    def share_heads():
        send("heads_c", heads.at[tp], heads.at[tp], c_dev)

    def relay_heads():
        receive("heads_x", heads.at[tp_x])
        send("heads_cx", heads.at[tp_x], heads.at[tp_x], c_dev)

    def await_heads():
        receive("heads_c", heads.at[tp_c])
        receive("heads_cx", heads.at[tp_c])

    def project(i):
        span = pl.ds(i * piece, piece)
        with NS(f"proj{i}"):
            joined = jnp.concatenate([heads[t, span] for t in range(4)], axis=1)
            mixed[span] = jnp.dot(joined, proj[...], preferred_element_type=jnp.float32).astype(
                jnp.bfloat16
            )

    gather_x(FIRST)
    gather_y(FIRST)
    depart("1")
    group_logits = lax.dot_general(
        group_ref[...], normed, across, preferred_element_type=jnp.float32
    )
    expert_logits = lax.dot_general(
        expert_ref[...], normed, across, preferred_element_type=jnp.float32
    )
    group_exp = jnp.exp(group_logits - jnp.max(group_logits, axis=0, keepdims=True))
    group_share = jnp.sum(jnp.where(named, group_exp, 0.0), axis=0, keepdims=True) / jnp.sum(
        group_exp, axis=0, keepdims=True
    )
    expert_at = lax.broadcasted_iota(jnp.int32, expert_logits.shape, 0)
    logit_a = jnp.sum(jnp.where(expert_at == route_a, expert_logits, 0.0), axis=0, keepdims=True)
    logit_b = jnp.sum(jnp.where(expert_at == route_b, expert_logits, 0.0), axis=0, keepdims=True)
    top = jnp.maximum(logit_a, logit_b)
    exp_a, exp_b = jnp.exp(logit_a - top), jnp.exp(logit_b - top)
    gate_a = group_share * (exp_a / (exp_a + exp_b))
    gate_b = group_share * (exp_b / (exp_a + exp_b))
    base = jnp.sum(jnp.where(named, group_at * group_experts, 0), axis=0, keepdims=True)
    slot_at = lax.broadcasted_iota(jnp.int32, (group_experts, block), 0)
    share_t = jnp.where(slot_at == route_a - base, gate_a, 0.0) + jnp.where(
        slot_at == route_b - base, gate_b, 0.0
    )
    coarse = share_t.astype(jnp.bfloat16)
    fine = (share_t - coarse.astype(jnp.float32)).astype(jnp.bfloat16)
    for i, piece_of in enumerate((coarse, fine)):
        share_ref[0, own, pl.ds(i * group_experts, group_experts)] = lax.dot_general(
            piece_of, take, across, preferred_element_type=jnp.float32
        ).astype(jnp.bfloat16)
    for step in range(1, groups):
        there = (plane(step) * 2 + member, tp)
        send("share_z", share_ref.at[0, own], share_ref.at[step, own], there)

    def spread_shares():
        receive("share_z", share_ref.at[pl.ds(1, groups - 1), own])
        mine_now = share_ref.at[:, own]
        for device in (d_dev, x_dev, y_dev):
            send("share", mine_now, mine_now, device)

    def swap_shares():
        receive("share", share_ref.at[:, pl.ds(mine, 3)])
        core_now = share_ref.at[:, mine_slots]
        send("share_c", core_now, core_now, c_dev)

    def take_shares():
        receive("share_c", share_ref.at[:, other_slots])

    with NS("wqkv"):
        for load in middle:
            load.wait()
    for name, ext in (("k", k_ext), ("v", v_ext)):
        send("halo" + name, ext.at[:, pl.ds(row_count, WINDOW)], ext.at[:, pl.ds(0, WINDOW)], next_dev)
    keep = pltpu.make_async_copy(
        xs_ref.at[pl.ds(my_start, chunk)], rows.at[0, own], out_sem.at[0]
    )
    keep.start()

    def take_halo():
        for name, ext in (("k", k_ext), ("v", v_ext)):
            receive("halo" + name, ext.at[:, pl.ds(0, WINDOW)])

    def take_weights():
        with NS("loads"):
            for load in late:
                load.wait()

    att(2, 4)
    send_heads(2, 4)
    att(4, 6)
    depart("c")
    depart("d")
    relay("0", 0)
    relay("0", 1)
    att(6, 7)
    spread_shares()
    arrive("1")
    gather_x("1")
    gather_y("1")
    att(7, 8)
    att(1, 2)
    take_halo()
    att(0, 1)
    share_heads()
    take_weights()
    keep.wait()
    core_near("0")
    core_far("0")
    swap_shares()
    relay("1", 0)
    relay("1", 1)
    depart("a")
    depart("b")
    core_near("1")
    arrive("c")
    gather_x("c")
    gather_y("c")
    arrive("d")
    gather_x("d")
    gather_y("d")
    send_heads(4, 6)
    take_shares()
    up("0", 0)
    up("0", 1)
    relay("c", 0)
    core_near("c")
    relay("d", 0)
    core_near("d")
    arrive("a")
    gather_x("a")
    gather_y("a")
    arrive("b")
    gather_x("b")
    gather_y("b")
    send_heads(6, 8)
    send_heads(0, 2)
    core_far("1")
    down("0")
    experts("1")
    relay("a", 0)
    core_near("a")
    core_far("c")
    relay("b", 0)
    core_near("b")
    core_far("d")
    scatter("1")
    experts("c")
    core_far("a")
    up("d", 0)
    up("d", 1)
    core_far("b")
    scatter("c")
    down("d")
    scatter_relay("1")
    relay_heads()
    up("a", 0)
    up("a", 1)
    scatter("d")
    down("a")
    scatter_relay("c")
    experts("b")
    scatter("a")
    await_heads()
    home("1")
    scatter("b")
    scatter_relay("d")
    project(0)
    home("c")
    project(1)
    scatter_relay("a")
    scatter_far("0")
    project(2)
    home("d")
    project(3)
    scatter_relay("b")
    scatter_near("0")
    home("a")
    scatter_relay("0")
    home("b")
    home("0")
    settle()
    with NS("wsend"):
        for copy in in_flight.values():
            copy.wait_send()


def store_kernel(mixed, back, take, mixer_hbm, out_hbm, moved, sem):
    mixer_copy = pltpu.make_async_copy(mixed, mixer_hbm, sem.at[0])
    mixer_copy.start()
    moved[...] = lax.dot_general(
        take[...], back[...], (((0,), (0,)), ((), ())), preferred_element_type=jnp.float32
    ).astype(jnp.bfloat16)
    out_copy = pltpu.make_async_copy(moved, out_hbm, sem.at[1])
    out_copy.start()
    mixer_copy.wait()
    out_copy.wait()


def store(mixed, back, take):
    anywhere = pl.BlockSpec(memory_space=pl.ANY)
    vmem = pl.BlockSpec(memory_space=pltpu.VMEM)
    return pl.pallas_call(
        store_kernel,
        out_shape=tuple(jax.ShapeDtypeStruct(v.shape, v.dtype) for v in (mixed, back)),
        in_specs=[anywhere, vmem, vmem],
        out_specs=(anywhere, anywhere),
        scratch_shapes=[pltpu.VMEM(back.shape, back.dtype), pltpu.SemaphoreType.DMA((2,))],
        compiler_params=pltpu.CompilerParams(vmem_limit_bytes=8 * 2**20),
    )(*(pltpu.with_memory_space_constraint(v, pltpu.VMEM) for v in (mixed, back, take)))


def fused(
    sinks,
    q_heads,
    k_heads,
    v_heads,
    gain,
    router_group,
    router_expert,
    routes,
    tokens_b,
    expert_gate,
    expert_up,
    expert_down,
    proj,
):
    groups = router_group.shape[1]
    block = tokens_b.shape[0] // 4
    experts, depth, hidden = expert_gate.shape
    row_count, head_width = q_heads.shape
    down = expert_down.reshape(experts * hidden, depth)
    chunk = block // groups
    bf16 = jnp.bfloat16
    anywhere = pl.BlockSpec(memory_space=pl.ANY)
    mixed, back, take = pl.pallas_call(
        functools.partial(fused_kernel, groups),
        out_shape=(
            pltpu.VMEM((row_count, proj.shape[1]), bf16),
            pltpu.VMEM((block, depth), bf16),
            pltpu.VMEM((block, block), bf16),
        ),
        in_specs=[anywhere] * 13,
        out_specs=(pl.BlockSpec(memory_space=pltpu.VMEM),) * 3,
        scratch_shapes=[
            pltpu.SMEM(sinks.shape, jnp.float32),
            pltpu.VMEM(q_heads.shape, bf16),
            pltpu.VMEM((1, depth), jnp.float32),
            pltpu.VMEM((groups, depth), bf16),
            pltpu.VMEM((router_expert.shape[1], depth), bf16),
            pltpu.VMEM((2, block), jnp.int32),
            pltpu.VMEM((HD, row_count + WINDOW), bf16),
            pltpu.VMEM((HD, row_count + WINDOW), bf16),
            pltpu.VMEM((block, depth), bf16),
            pltpu.VMEM((block, depth), bf16),
            pltpu.VMEM((groups, 8, 2 * (router_expert.shape[1] // groups), block), bf16),
            pltpu.VMEM((4, row_count, head_width), bf16),
            pltpu.VMEM((groups, 8, chunk, depth), bf16),
            pltpu.VMEM((groups, 8, chunk, depth), bf16),
            pltpu.VMEM(expert_gate.shape, bf16),
            pltpu.VMEM(expert_up.shape, bf16),
            pltpu.VMEM(down.shape, bf16),
            pltpu.VMEM(proj.shape, bf16),
            pltpu.VMEM((experts, 8 * chunk, hidden), bf16),
            pltpu.VMEM((groups, 4, chunk, depth), bf16),
            pltpu.VMEM((groups, chunk, depth // 2), bf16),
            pltpu.VMEM((groups, chunk, depth // 2), bf16),
            pltpu.VMEM((groups, 2, chunk, depth), bf16),
            pltpu.VMEM((groups, chunk, depth), bf16),
            pltpu.SemaphoreType.DMA((13,)),
            pltpu.SemaphoreType.DMA((1,)),
            pltpu.SemaphoreType.DMA((SENDERS,)),
            pltpu.SemaphoreType.DMA((RECEIVERS,)),
        ],
        cost_estimate=pl.CostEstimate(
            flops=20_000_000_000, bytes_accessed=20_000_000, transcendentals=0
        ),
        compiler_params=pltpu.CompilerParams(
            collective_id=0, has_side_effects=True, vmem_limit_bytes=40 * 2**20
        ),
    )(
        *(
            pltpu.with_memory_space_constraint(value, pltpu.HBM)
            for value in (
                sinks,
                q_heads,
                k_heads.T,
                v_heads.T,
                gain[None, :],
                router_group.T,
                router_expert.T,
                routes.T,
                tokens_b,
                expert_gate,
                expert_up,
                down,
                proj,
            )
        )
    )
    return store(mixed, back, take)


def per_device(
    q_heads,
    k_heads,
    v_heads,
    sink_logits,
    out_weight,
    tokens_b,
    moe_gain,
    router_group,
    router_expert,
    route_expert,
    expert_gate,
    expert_up,
    expert_down,
):
    groups = router_group.shape[1]
    if (lax.axis_size("ep"), lax.axis_size("tp"), k_heads.shape[1]) == (2 * groups, 4, HD):
        return fused(
            sink_logits,
            q_heads,
            k_heads,
            v_heads,
            moe_gain,
            router_group,
            router_expert,
            route_expert,
            tokens_b,
            expert_gate,
            expert_up,
            expert_down,
            out_weight,
        )
    span_len = WINDOW
    row_count = q_heads.shape[0]
    kv_local = k_heads.shape[1] // HD
    group_size = HEADS // KV
    blocks = row_count // span_len
    stacked = jnp.stack([k_heads[row_count - span_len :], v_heads[row_count - span_len :]])
    earlier = shifted(stacked, "ep", 1)

    def make_band(own_rows, prev_rows):
        extended = jnp.concatenate([prev_rows, own_rows], axis=0).reshape(
            blocks + 1, span_len, kv_local, HD
        )
        return jnp.concatenate([extended[:-1], extended[1:]], axis=1)

    key_band = make_band(k_heads, earlier[0])
    value_band = make_band(v_heads, earlier[1])
    query_blocks = q_heads.reshape(blocks, span_len, kv_local, group_size, HD)
    scores = jnp.einsum(
        "nqhgd,nkhd->nhgqk", query_blocks, key_band, preferred_element_type=jnp.float32
    ) * HD ** (-0.5)
    first_row = lax.axis_index("ep") * row_count
    query_index = jnp.arange(span_len, dtype=jnp.int32)[:, None]
    key_index = jnp.arange(2 * span_len, dtype=jnp.int32)[None, :]
    distance = query_index + span_len - key_index
    key_place = (
        first_row
        + jnp.arange(blocks, dtype=jnp.int32)[:, None, None] * span_len
        + key_index[None]
        - span_len
    )
    allowed = (distance >= 0)[None] & (distance < span_len)[None] & (key_place >= 0)
    masked = jnp.where(allowed[:, None, None], scores, -1e30)
    sink_full = sink_logits.reshape(kv_local, group_size)[None, :, :, None]
    row_max = jnp.maximum(jnp.max(masked, axis=-1), sink_full)
    weights_exp = jnp.exp(masked - row_max[..., None])
    denominator = jnp.sum(weights_exp, axis=-1) + jnp.exp(sink_full - row_max)
    probs = (weights_exp / denominator[..., None]).astype(jnp.bfloat16)
    attended = jnp.einsum(
        "nhgqk,nkhd->nqhgd", probs, value_band, preferred_element_type=jnp.float32
    )
    attended = attended.astype(jnp.bfloat16).reshape(row_count, kv_local * group_size * HD)
    mixed = jnp.dot(
        lax.all_gather(attended, "tp", axis=1, tiled=True),
        out_weight,
        preferred_element_type=jnp.float32,
    )
    mixer_out = mixed.astype(jnp.bfloat16)
    tp_count = lax.axis_size("tp")
    tp_index = lax.axis_index("tp")
    exp_local = expert_gate.shape[0]
    expert_count = exp_local * lax.axis_size("ep")
    rows_dev = tokens_b.shape[0] // tp_count
    capacity = min(4 * rows_dev // expert_count, rows_dev // 4)
    own_routes = lax.dynamic_slice_in_dim(route_expert, tp_index * rows_dev, rows_dev, 0)
    own_normed = normalize(
        lax.dynamic_slice_in_dim(tokens_b, tp_index * rows_dev, rows_dev, 0), moe_gain
    )
    flat_routes, places = slot_positions(own_routes, 1, expert_count)
    buffer = fill_slots(own_normed, flat_routes, places, 1, expert_count, capacity, exp_local)
    delivered = lax.all_to_all(buffer, "ep", split_axis=0, concat_axis=0, tiled=True)
    arrived = lax.all_gather(delivered, "tp", axis=2, tiled=True)
    own_flat = flat_routes[0]
    own_places = places[0]
    gates = gate_weights(own_normed, own_routes, router_group, router_expert)
    gate_pre = jnp.einsum(
        "setcd,edf->setcf", arrived, expert_gate, preferred_element_type=jnp.float32
    )
    up_pre = jnp.einsum("setcd,edf->setcf", arrived, expert_up, preferred_element_type=jnp.float32)
    activated = (jax.nn.silu(gate_pre) * up_pre).astype(jnp.bfloat16)
    partial_value = jnp.einsum(
        "setcf,efd->setcd", activated, expert_down, preferred_element_type=jnp.float32
    )
    summed = lax.psum_scatter(
        partial_value.astype(jnp.bfloat16), "tp", scatter_dimension=2, tiled=True
    )
    returned = lax.all_to_all(summed, "ep", split_axis=0, concat_axis=0, tiled=True)
    returned = returned.reshape(expert_count * capacity, returned.shape[-1])
    picked_rows = returned[own_flat * capacity + own_places].reshape(
        rows_dev, 2, returned.shape[-1]
    )
    moe_out = jnp.sum(gates[:, :, None] * picked_rows.astype(jnp.float32), axis=1).astype(
        jnp.bfloat16
    )
    return (mixer_out, moe_out)


def solution(mesh):
    in_specs = (
        P("ep", "tp"),
        P("ep", "tp"),
        P("ep", "tp"),
        P("tp"),
        P(None, "tp"),
        P("ep", None),
        P(),
        P(),
        P(),
        P("ep", None),
        P("ep", None, "tp"),
        P("ep", None, "tp"),
        P("ep", "tp", None),
    )
    out_specs = (P("ep", "tp"), P(("ep", "tp"), None))
    return jax.shard_map(
        per_device, mesh=mesh, in_specs=in_specs, out_specs=out_specs, check_vma=False
    )
```

```python
import contextlib
import functools

import jax
import jax.numpy as jnp
from jax import lax
from jax.experimental import pallas as pl
from jax.experimental.pallas import tpu as pltpu
from jax.sharding import PartitionSpec as P

HEADS = 16
KV = 4
HD = 64
WINDOW = 128


def shifted(value, axis, steps):
    count = lax.axis_size(axis)
    leading, last = (max(0, -steps), min(count, count - steps))
    return lax.ppermute(value, axis, [(source, source + steps) for source in range(leading, last)])


def normalize(rows_in, gain):
    values = rows_in.astype(jnp.float32)
    scaled = values * lax.rsqrt(jnp.mean(values * values, axis=-1, keepdims=True) + 1e-06) * gain
    return scaled.astype(jnp.bfloat16)


def gate_weights(normed, routes, router_group, router_expert):
    group_logits = jnp.dot(normed, router_group, preferred_element_type=jnp.float32)
    expert_logits = jnp.dot(normed, router_expert, preferred_element_type=jnp.float32)
    group_count = router_group.shape[1]
    expert_count = router_expert.shape[1]
    chosen_group = routes[:, 0] // (expert_count // group_count)
    group_match = chosen_group[:, None] == jnp.arange(group_count, dtype=jnp.int32)[None, :]
    group_share = jnp.sum(
        jnp.where(group_match, jax.nn.softmax(group_logits, axis=-1), 0.0), axis=-1
    )
    expert_match = routes[:, :, None] == jnp.arange(expert_count, dtype=jnp.int32)[None, None, :]
    picked = jnp.sum(jnp.where(expert_match, expert_logits[:, None, :], 0.0), axis=-1)
    return group_share[:, None] * jax.nn.softmax(picked, axis=-1)


def slot_positions(routes, sub_count, expert_count):
    flat_routes = routes.reshape(sub_count, -1)
    onehot = (
        flat_routes[:, :, None] == jnp.arange(expert_count, dtype=jnp.int32)[None, None, :]
    ).astype(jnp.int32)
    places = jnp.sum(onehot * jnp.cumsum(onehot, axis=1), axis=2) - 1
    return (flat_routes, places)


def fill_slots(normed, flat_routes, places, sub_count, expert_count, capacity, exp_local):
    sub_index = jnp.arange(sub_count, dtype=jnp.int32)[:, None]
    target = ((flat_routes * sub_count + sub_index) * capacity + places).reshape(-1)
    source = jnp.repeat(normed, 2, axis=0)
    buffer = jnp.zeros((expert_count * sub_count * capacity, normed.shape[1]), jnp.bfloat16)
    buffer = buffer.at[target].set(source)
    return buffer.reshape(
        expert_count // exp_local, exp_local, sub_count, capacity, normed.shape[1]
    )


LANES = 128
MESH = pl.DeviceIdType.MESH


@contextlib.contextmanager
def NS(name):
    pl.delay(1)
    yield
    pl.delay(1)

FIRST = "0"
SENDERS = 24
RECEIVERS = 58


def UNITS(chunk):
    half = chunk // 2
    return {
        "0": (0, 0, chunk),
        "1": (1, 0, chunk),
        "c": (2, 0, half),
        "d": (2, half, half),
        "a": (3, 0, half),
        "b": (3, half, half),
    }


def fused_kernel(
    groups,
    sink_hbm,
    q_hbm,
    k_hbm,
    v_hbm,
    gain_hbm,
    group_hbm,
    expert_hbm,
    route_hbm,
    tokens_hbm,
    gate_hbm,
    up_hbm,
    down_hbm,
    proj_hbm,
    mixed,
    back,
    take_out,
    sink_ref,
    q_ref,
    gain_ref,
    group_ref,
    expert_ref,
    route_ref,
    k_ext,
    v_ext,
    tokens,
    xs_ref,
    share_ref,
    heads,
    rows,
    part,
    wg,
    wu,
    wd,
    proj,
    act,
    from_core,
    relay_x,
    relay_y,
    from_xy,
    total,
    load_sem,
    out_sem,
    send_sem,
    recv_sem,
):
    ep, tp = lax.axis_index("ep"), lax.axis_index("tp")
    group, member = ep // 2, ep % 2
    x, core = tp // 2, tp % 2
    tp_x, tp_c = (1 - x) * 2 + core, x * 2 + (1 - core)
    ep_y = group * 2 + (1 - member)
    ep_count = groups * 2
    x_dev, y_dev, c_dev, d_dev = (ep, tp_x), (ep_y, tp), (ep, tp_c), (ep_y, tp_x)
    next_dev = ((ep + 1) % ep_count, tp)
    prev_dev = ((ep + ep_count - 1) % ep_count, tp)
    depth = back.shape[1]
    block = xs_ref.shape[0]
    chunk = block // groups
    row_count = q_ref.shape[0]
    mine, other = core * 4, (1 - core) * 4
    own = mine + member * 2 + x
    slot_x = mine + member * 2 + (1 - x)
    slot_y = mine + (1 - member) * 2 + x
    slot_d = mine + (1 - member) * 2 + (1 - x)
    mine_slots, other_slots = pl.ds(mine, 4), pl.ds(other, 4)

    def plane(step):
        return (group + step) % groups

    barrier = pltpu.get_barrier_semaphore()
    ahead = [plane(step) * 2 + member for step in range(1, groups)]
    peers = [(there, tp) for there in ahead] + [x_dev, y_dev, c_dev, d_dev, next_dev, prev_dev]
    for peer in peers:
        pl.semaphore_signal(barrier, inc=1, device_id=peer, device_id_type=MESH)

    first = pl.multiple_of(tp * block, block)
    inner = pl.ds(WINDOW, row_count)
    pairs = (
        (tokens_hbm.at[pl.ds(first, block)], tokens),
        (gain_hbm, gain_ref),
        (group_hbm, group_ref),
        (expert_hbm, expert_ref),
        (route_hbm.at[:, pl.ds(first, block)], route_ref),
        (k_hbm, k_ext.at[:, inner]),
        (v_hbm, v_ext.at[:, inner]),
        (q_hbm, q_ref),
        (sink_hbm, sink_ref),
        (gate_hbm, wg),
        (up_hbm, wu),
        (down_hbm, wd),
        (proj_hbm, proj),
    )
    loads = [
        pltpu.make_async_copy(source, held, load_sem.at[i])
        for i, (source, held) in enumerate(pairs)
    ]
    early, middle, late = loads[:5], loads[5:9], loads[9:]
    for load in early:
        load.start()
    early[4].wait()
    routes = route_ref[...]
    route_a, route_b = routes[0:1], routes[1:2]
    group_experts = expert_ref.shape[0] // groups
    group_at = lax.broadcasted_iota(jnp.int32, (groups, block), 0)
    inside = route_a - group_at * group_experts
    named = (inside >= 0) & (inside < group_experts)
    row_at = lax.broadcasted_iota(jnp.int32, (block, block), 0)
    column_at = lax.broadcasted_iota(jnp.int32, (block, block), 1)
    earlier = jnp.where(row_at < column_at, 1.0, 0.0).astype(jnp.bfloat16)
    counts = jnp.dot(
        jnp.where(named, 1.0, 0.0).astype(jnp.bfloat16), earlier, preferred_element_type=jnp.float32
    )
    first_row = (group_at * chunk).astype(jnp.float32)
    place = jnp.sum(jnp.where(named, counts + first_row, 0.0), axis=0, keepdims=True)
    take = jnp.where(row_at.astype(jnp.float32) == place, 1.0, 0.0).astype(jnp.bfloat16)
    with NS("wearly"):
        for load in early[:4]:
            load.wait()
    for load in middle + late:
        load.start()
    values = tokens[...].astype(jnp.float32)
    scale = lax.rsqrt(jnp.mean(values * values, axis=1, keepdims=True) + 1e-06)
    normed = (values * scale * gain_ref[...]).astype(jnp.bfloat16)
    across = (((1,), (1,)), ((), ()))
    xs_ref[...] = jnp.dot(take, normed, preferred_element_type=jnp.float32).astype(jnp.bfloat16)
    take_out[...] = take
    with NS("barrier"):
        pl.semaphore_wait(barrier, len(peers))

    in_flight, used, names = {}, [0], {}

    def descriptor(source, target, device, sender, name):
        receiver = names.setdefault(name, len(names))
        return pltpu.make_async_remote_copy(
            src_ref=source,
            dst_ref=target,
            send_sem=send_sem.at[sender],
            recv_sem=recv_sem.at[receiver],
            device_id=device,
            device_id_type=MESH,
        )

    def send(name, source, target, device):
        sender = used[0] % send_sem.shape[0]
        used[0] += 1
        if sender in in_flight:
            in_flight[sender].wait_send()
        copy = descriptor(source, target, device, sender, name)
        copy.start()
        in_flight[sender] = copy

    def receive(name, target, scope=None):
        with NS(scope or "w" + name):
            descriptor(target, target, x_dev, 0, name).wait_recv()

    my_start = pl.multiple_of(group * chunk, chunk)
    units = UNITS(chunk)
    piece_rows = 16
    near_pair = pl.ds(mine + member * 2, 2)
    far_pair = pl.ds(mine + (1 - member) * 2, 2)
    width_half = depth // 2
    sides = (pl.ds(0, width_half), pl.ds(width_half, width_half))

    def span_of(u):
        return pl.ds(units[u][1], units[u][2])

    def own_rows(s, begin, count):
        if s == 0:
            return xs_ref.at[pl.ds(pl.multiple_of(my_start + begin, piece_rows), count)]
        return rows.at[s, own, pl.ds(begin, count)]

    def depart(u):
        s, begin, count = units[u]
        if s:
            there = pl.ds(pl.multiple_of(plane(s) * chunk + begin, piece_rows), count)
            send(f"z{u}", xs_ref.at[there], rows.at[s, own, span_of(u)], (plane(s) * 2 + member, tp))

    def arrive(u):
        s = units[u][0]
        receive(f"z{u}", rows.at[s, own, span_of(u)])

    def gather_x(u):
        for i in range(units[u][2] // piece_rows):
            gather_piece(u, i)

    def gather_piece(u, i):
        s, begin, count = units[u]
        at = begin + i * piece_rows
        target = rows.at[s, own, pl.ds(at, piece_rows)]
        send(f"x{u}{i}", own_rows(s, at, piece_rows), target, x_dev)

    def gather_y(u):
        s, begin, count = units[u]
        send(f"y{u}", own_rows(s, begin, count), rows.at[s, own, span_of(u)], y_dev)

    def relay(u, i):
        s, begin, count = units[u]
        block_at = rows.at[s, slot_x, pl.ds(begin + i * piece_rows, piece_rows)]
        receive(f"x{u}{i}", block_at)
        send(f"y{u}", block_at, block_at, y_dev)

    def core_near(u):
        s = units[u][0]
        pair = rows.at[s, near_pair, span_of(u)]
        send(f"core{u}", pair, pair, c_dev)

    def core_far(u):
        s = units[u][0]
        pair = rows.at[s, far_pair, span_of(u)]
        receive(f"y{u}", pair)
        send(f"core{u}", pair, pair, c_dev)

    def up(u, e):
        s, begin, count = units[u]
        if e == 0:
            receive(f"core{u}", rows.at[s, other_slots, span_of(u)])
        batch = 8 * count
        with NS(f"up{u}{e}"):
            tokens = rows[s, :, begin : begin + count].reshape(batch, depth)
            held = share_ref[s].astype(jnp.float32)
            at = lax.broadcasted_iota(jnp.int32, held.shape, 1) % group_experts
            wanted = at == member * wg.shape[0] + e
            by_lane = jnp.sum(jnp.where(wanted, held, 0.0), axis=1, keepdims=True)
            shape = (8, count, block)
            lane = lax.broadcasted_iota(jnp.int32, shape, 2) - group * chunk - begin
            picked = lane == lax.broadcasted_iota(jnp.int32, shape, 1)
            share = jnp.sum(
                jnp.where(picked, jnp.broadcast_to(by_lane, shape), 0.0), axis=2, keepdims=True
            ).reshape(batch, 1)
            pre = jnp.dot(tokens, wg[e], preferred_element_type=jnp.float32)
            high = jnp.dot(tokens, wu[e], preferred_element_type=jnp.float32)
            act[e, :batch] = (jax.nn.silu(pre) * high * share).astype(jnp.bfloat16)

    def down(u):
        s, begin, count = units[u]
        batch = 8 * count
        tile = 512
        acts = jnp.concatenate([act[e, :batch] for e in range(wg.shape[0])], axis=1)

        def column(n, carry):
            columns = pl.ds(pl.multiple_of(n * tile, tile), tile)
            value = jnp.dot(acts, wd[:, columns], preferred_element_type=jnp.float32)
            part[s, :, begin : begin + count, columns] = value.astype(jnp.bfloat16).reshape(
                8, count, tile
            )
            return carry

        with NS(f"down{u}"):
            for i, side in enumerate(sides):
                tiles = width_half // tile
                lax.fori_loop(i * tiles, (i + 1) * tiles, column, 0)
                send(
                    f"sum{u}",
                    part.at[s, other_slots, span_of(u), side],
                    from_core.at[s, :, span_of(u), side],
                    c_dev,
                )

    def experts(u):
        for e in range(wg.shape[0]):
            up(u, e)
        down(u)

    def add(index, term):
        part[index] = (part[index].astype(jnp.float32) + term.astype(jnp.float32)).astype(
            jnp.bfloat16
        )

    def scatter(u):
        scatter_far(u)
        scatter_near(u)

    def scatter_far(u):
        s, begin, count = units[u]
        span = span_of(u)
        left, right = sides
        receive(f"sum{u}", from_core.at[s, :, span])
        with NS(f"E{u}"):
            add((s, mine_slots, span), from_core[s, :, span])
        send(f"dy{u}", part.at[s, slot_d, span, left], relay_y.at[s, span], y_dev)
        send(f"dx{u}", part.at[s, slot_d, span, right], relay_x.at[s, span], x_dev)

    def scatter_near(u):
        s, begin, count = units[u]
        span = span_of(u)
        left, right = sides
        send(f"xy{u}", part.at[s, slot_x, span, right], from_xy.at[s, 0, span, right], x_dev)
        send(f"xy{u}", part.at[s, slot_y, span, left], from_xy.at[s, 1, span, left], y_dev)

    def scatter_relay(u):
        s, begin, count = units[u]
        span = span_of(u)
        left, right = sides
        receive(f"dy{u}", relay_y.at[s, span])
        add((s, slot_x, span, left), relay_y[s, span])
        send(f"xy{u}", part.at[s, slot_x, span, left], from_xy.at[s, 0, span, left], x_dev)
        receive(f"dx{u}", relay_x.at[s, span])
        add((s, slot_y, span, right), relay_x[s, span])
        send(f"xy{u}", part.at[s, slot_y, span, right], from_xy.at[s, 1, span, right], y_dev)

    def home(u):
        s, begin, count = units[u]
        span = span_of(u)
        receive(f"xy{u}", from_xy.at[s, :, span], f"wH{u}")
        summed = (
            part[s, own, span].astype(jnp.float32)
            + from_xy[s, 0, span].astype(jnp.float32)
            + from_xy[s, 1, span].astype(jnp.float32)
        ).astype(jnp.bfloat16)
        there = pl.ds(pl.multiple_of(my_start + begin, piece_rows), count)
        if s:
            total[s, span] = summed
            to = (group + groups - s) % groups
            send("home", total.at[s, span], back.at[there], (to * 2 + member, tp))
        else:
            back[there] = summed

    def settle():
        receive("home", back.at[pl.ds(0, block - chunk)])

    head_count = q_ref.shape[1] // HD
    query_at = lax.broadcasted_iota(jnp.int32, (WINDOW, 2 * WINDOW), 0)
    key_at = lax.broadcasted_iota(jnp.int32, (WINDOW, 2 * WINDOW), 1)
    distance = query_at + WINDOW - key_at
    near = (distance >= 0) & (distance < WINDOW)

    def attend(b, carry):
        start = pl.multiple_of(b * WINDOW, WINDOW)
        keys = k_ext[:, pl.ds(start, 2 * WINDOW)]
        band = v_ext[:, pl.ds(start, 2 * WINDOW)]
        queries = q_ref[pl.ds(start, WINDOW)]
        allowed = near & (key_at + (ep * row_count + b * WINDOW - WINDOW) >= 0)
        outs = []
        for h in range(head_count):
            query = queries[:, h * HD : (h + 1) * HD]
            scores = jnp.dot(query, keys, preferred_element_type=jnp.float32) * HD ** (-0.5)
            masked = jnp.where(allowed, scores, -1e30)
            sink = jnp.full((WINDOW, 1), sink_ref[h], jnp.float32)
            row_max = jnp.maximum(jnp.max(masked, axis=1, keepdims=True), sink)
            weights = jnp.exp(masked - row_max)
            denominator = jnp.sum(weights, axis=1, keepdims=True) + jnp.exp(sink - row_max)
            probs = (weights * (1.0 / denominator)).astype(jnp.bfloat16)
            outs.append(lax.dot_general(probs, band, across, preferred_element_type=jnp.float32))
        heads[tp, pl.ds(start, WINDOW)] = jnp.concatenate(outs, axis=1).astype(jnp.bfloat16)
        return carry

    def att(first_block, last_block):
        with NS(f"att{first_block}"):
            lax.fori_loop(first_block, last_block, attend, 0)

    blocks = row_count // WINDOW
    pieces = 4
    piece = row_count // pieces

    def send_heads(begin, end):
        span = pl.ds(begin * WINDOW, (end - begin) * WINDOW)
        send("heads_x", heads.at[tp, span], heads.at[tp, span], x_dev)

    def share_heads():
        send("heads_c", heads.at[tp], heads.at[tp], c_dev)

    def relay_heads():
        receive("heads_x", heads.at[tp_x])
        send("heads_cx", heads.at[tp_x], heads.at[tp_x], c_dev)

    def await_heads():
        receive("heads_c", heads.at[tp_c])
        receive("heads_cx", heads.at[tp_c])

    def project(i):
        span = pl.ds(i * piece, piece)
        with NS(f"proj{i}"):
            joined = jnp.concatenate([heads[t, span] for t in range(4)], axis=1)
            mixed[span] = jnp.dot(joined, proj[...], preferred_element_type=jnp.float32).astype(
                jnp.bfloat16
            )

    gather_piece(FIRST, 0)
    gather_y(FIRST)
    depart("1")
    group_logits = lax.dot_general(
        group_ref[...], normed, across, preferred_element_type=jnp.float32
    )
    expert_logits = lax.dot_general(
        expert_ref[...], normed, across, preferred_element_type=jnp.float32
    )
    group_exp = jnp.exp(group_logits - jnp.max(group_logits, axis=0, keepdims=True))
    group_share = jnp.sum(jnp.where(named, group_exp, 0.0), axis=0, keepdims=True) / jnp.sum(
        group_exp, axis=0, keepdims=True
    )
    expert_at = lax.broadcasted_iota(jnp.int32, expert_logits.shape, 0)
    logit_a = jnp.sum(jnp.where(expert_at == route_a, expert_logits, 0.0), axis=0, keepdims=True)
    logit_b = jnp.sum(jnp.where(expert_at == route_b, expert_logits, 0.0), axis=0, keepdims=True)
    top = jnp.maximum(logit_a, logit_b)
    exp_a, exp_b = jnp.exp(logit_a - top), jnp.exp(logit_b - top)
    gate_a = group_share * (exp_a / (exp_a + exp_b))
    gate_b = group_share * (exp_b / (exp_a + exp_b))
    base = jnp.sum(jnp.where(named, group_at * group_experts, 0), axis=0, keepdims=True)
    slot_at = lax.broadcasted_iota(jnp.int32, (group_experts, block), 0)
    share_t = jnp.where(slot_at == route_a - base, gate_a, 0.0) + jnp.where(
        slot_at == route_b - base, gate_b, 0.0
    )
    coarse = share_t.astype(jnp.bfloat16)
    fine = (share_t - coarse.astype(jnp.float32)).astype(jnp.bfloat16)
    for i, piece_of in enumerate((coarse, fine)):
        share_ref[0, own, pl.ds(i * group_experts, group_experts)] = lax.dot_general(
            piece_of, take, across, preferred_element_type=jnp.float32
        ).astype(jnp.bfloat16)
    for step in range(1, groups):
        there = (plane(step) * 2 + member, tp)
        send("share_z", share_ref.at[0, own], share_ref.at[step, own], there)

    gather_piece(FIRST, 1)

    def spread_shares():
        receive("share_z", share_ref.at[pl.ds(1, groups - 1), own])
        mine_now = share_ref.at[:, own]
        for device in (d_dev, x_dev, y_dev):
            send("share", mine_now, mine_now, device)

    def swap_shares():
        receive("share", share_ref.at[:, pl.ds(mine, 3)])
        core_now = share_ref.at[:, mine_slots]
        send("share_c", core_now, core_now, c_dev)

    def take_shares():
        receive("share_c", share_ref.at[:, other_slots])

    with NS("wqkv"):
        for load in middle:
            load.wait()
    for name, ext in (("k", k_ext), ("v", v_ext)):
        send("halo" + name, ext.at[:, pl.ds(row_count, WINDOW)], ext.at[:, pl.ds(0, WINDOW)], next_dev)
    keep = pltpu.make_async_copy(
        xs_ref.at[pl.ds(my_start, chunk)], rows.at[0, own], out_sem.at[0]
    )
    keep.start()

    def take_halo():
        for name, ext in (("k", k_ext), ("v", v_ext)):
            receive("halo" + name, ext.at[:, pl.ds(0, WINDOW)])

    def take_weights():
        with NS("loads"):
            for load in late:
                load.wait()

    att(2, 4)
    send_heads(2, 4)
    att(4, 6)
    depart("c")
    depart("d")
    relay("0", 0)
    relay("0", 1)
    att(6, 7)
    spread_shares()
    arrive("1")
    gather_x("1")
    gather_y("1")
    att(7, 8)
    att(1, 2)
    take_halo()
    att(0, 1)
    share_heads()
    take_weights()
    keep.wait()
    core_near("0")
    send_heads(4, 6)
    core_far("0")
    swap_shares()
    relay("1", 0)
    relay("1", 1)
    depart("a")
    depart("b")
    core_near("1")
    arrive("c")
    gather_x("c")
    gather_y("c")
    arrive("d")
    gather_x("d")
    gather_y("d")
    take_shares()
    up("0", 0)
    up("0", 1)
    relay("c", 0)
    core_near("c")
    relay("d", 0)
    core_near("d")
    arrive("a")
    gather_x("a")
    gather_y("a")
    arrive("b")
    gather_x("b")
    gather_y("b")
    send_heads(6, 8)
    send_heads(0, 2)
    core_far("1")
    down("0")
    up("1", 0)
    up("1", 1)
    down("1")
    relay("a", 0)
    core_near("a")
    core_far("c")
    relay("b", 0)
    core_near("b")
    core_far("d")
    scatter_far("1")
    scatter_near("1")
    up("c", 0)
    up("c", 1)
    down("c")
    core_far("a")
    up("d", 0)
    up("d", 1)
    core_far("b")
    scatter_far("c")
    down("d")
    scatter_relay("1")
    scatter_near("c")
    relay_heads()
    up("a", 0)
    up("a", 1)
    scatter_far("d")
    scatter_near("d")
    down("a")
    scatter_relay("c")
    up("b", 0)
    up("b", 1)
    scatter_far("a")
    scatter_near("a")
    down("b")
    await_heads()
    home("1")
    scatter_far("b")
    scatter_near("b")
    scatter_relay("d")
    project(0)
    home("c")
    scatter_far("0")
    project(1)
    project(3)
    scatter_relay("a")
    project(2)
    home("d")
    scatter_relay("b")
    scatter_near("0")
    home("a")
    scatter_relay("0")
    home("b")
    home("0")
    settle()
    with NS("wsend"):
        for copy in in_flight.values():
            copy.wait_send()


def store_kernel(mixed, back, take, mixer_hbm, out_hbm, moved, sem):
    mixer_copy = pltpu.make_async_copy(mixed, mixer_hbm, sem.at[0])
    mixer_copy.start()
    moved[...] = lax.dot_general(
        take[...], back[...], (((0,), (0,)), ((), ())), preferred_element_type=jnp.float32
    ).astype(jnp.bfloat16)
    out_copy = pltpu.make_async_copy(moved, out_hbm, sem.at[1])
    out_copy.start()
    mixer_copy.wait()
    out_copy.wait()


def store(mixed, back, take):
    anywhere = pl.BlockSpec(memory_space=pl.ANY)
    vmem = pl.BlockSpec(memory_space=pltpu.VMEM)
    return pl.pallas_call(
        store_kernel,
        out_shape=tuple(jax.ShapeDtypeStruct(v.shape, v.dtype) for v in (mixed, back)),
        in_specs=[anywhere, vmem, vmem],
        out_specs=(anywhere, anywhere),
        scratch_shapes=[pltpu.VMEM(back.shape, back.dtype), pltpu.SemaphoreType.DMA((2,))],
        compiler_params=pltpu.CompilerParams(vmem_limit_bytes=8 * 2**20),
    )(*(pltpu.with_memory_space_constraint(v, pltpu.VMEM) for v in (mixed, back, take)))


def fused(
    sinks,
    q_heads,
    k_heads,
    v_heads,
    gain,
    router_group,
    router_expert,
    routes,
    tokens_b,
    expert_gate,
    expert_up,
    expert_down,
    proj,
):
    groups = router_group.shape[1]
    block = tokens_b.shape[0] // 4
    experts, depth, hidden = expert_gate.shape
    row_count, head_width = q_heads.shape
    down = expert_down.reshape(experts * hidden, depth)
    chunk = block // groups
    bf16 = jnp.bfloat16
    anywhere = pl.BlockSpec(memory_space=pl.ANY)
    mixed, back, take = pl.pallas_call(
        functools.partial(fused_kernel, groups),
        out_shape=(
            pltpu.VMEM((row_count, proj.shape[1]), bf16),
            pltpu.VMEM((block, depth), bf16),
            pltpu.VMEM((block, block), bf16),
        ),
        in_specs=[anywhere] * 13,
        out_specs=(pl.BlockSpec(memory_space=pltpu.VMEM),) * 3,
        scratch_shapes=[
            pltpu.SMEM(sinks.shape, jnp.float32),
            pltpu.VMEM(q_heads.shape, bf16),
            pltpu.VMEM((1, depth), jnp.float32),
            pltpu.VMEM((groups, depth), bf16),
            pltpu.VMEM((router_expert.shape[1], depth), bf16),
            pltpu.VMEM((2, block), jnp.int32),
            pltpu.VMEM((HD, row_count + WINDOW), bf16),
            pltpu.VMEM((HD, row_count + WINDOW), bf16),
            pltpu.VMEM((block, depth), bf16),
            pltpu.VMEM((block, depth), bf16),
            pltpu.VMEM((groups, 8, 2 * (router_expert.shape[1] // groups), block), bf16),
            pltpu.VMEM((4, row_count, head_width), bf16),
            pltpu.VMEM((groups, 8, chunk, depth), bf16),
            pltpu.VMEM((groups, 8, chunk, depth), bf16),
            pltpu.VMEM(expert_gate.shape, bf16),
            pltpu.VMEM(expert_up.shape, bf16),
            pltpu.VMEM(down.shape, bf16),
            pltpu.VMEM(proj.shape, bf16),
            pltpu.VMEM((experts, 8 * chunk, hidden), bf16),
            pltpu.VMEM((groups, 4, chunk, depth), bf16),
            pltpu.VMEM((groups, chunk, depth // 2), bf16),
            pltpu.VMEM((groups, chunk, depth // 2), bf16),
            pltpu.VMEM((groups, 2, chunk, depth), bf16),
            pltpu.VMEM((groups, chunk, depth), bf16),
            pltpu.SemaphoreType.DMA((13,)),
            pltpu.SemaphoreType.DMA((1,)),
            pltpu.SemaphoreType.DMA((SENDERS,)),
            pltpu.SemaphoreType.DMA((RECEIVERS,)),
        ],
        cost_estimate=pl.CostEstimate(
            flops=20_000_000_000, bytes_accessed=20_000_000, transcendentals=0
        ),
        compiler_params=pltpu.CompilerParams(
            collective_id=0, has_side_effects=True, vmem_limit_bytes=40 * 2**20
        ),
    )(
        *(
            pltpu.with_memory_space_constraint(value, pltpu.HBM)
            for value in (
                sinks,
                q_heads,
                k_heads.T,
                v_heads.T,
                gain[None, :],
                router_group.T,
                router_expert.T,
                routes.T,
                tokens_b,
                expert_gate,
                expert_up,
                down,
                proj,
            )
        )
    )
    return store(mixed, back, take)


def per_device(
    q_heads,
    k_heads,
    v_heads,
    sink_logits,
    out_weight,
    tokens_b,
    moe_gain,
    router_group,
    router_expert,
    route_expert,
    expert_gate,
    expert_up,
    expert_down,
):
    groups = router_group.shape[1]
    if (lax.axis_size("ep"), lax.axis_size("tp"), k_heads.shape[1]) == (2 * groups, 4, HD):
        return fused(
            sink_logits,
            q_heads,
            k_heads,
            v_heads,
            moe_gain,
            router_group,
            router_expert,
            route_expert,
            tokens_b,
            expert_gate,
            expert_up,
            expert_down,
            out_weight,
        )
    span_len = WINDOW
    row_count = q_heads.shape[0]
    kv_local = k_heads.shape[1] // HD
    group_size = HEADS // KV
    blocks = row_count // span_len
    stacked = jnp.stack([k_heads[row_count - span_len :], v_heads[row_count - span_len :]])
    earlier = shifted(stacked, "ep", 1)

    def make_band(own_rows, prev_rows):
        extended = jnp.concatenate([prev_rows, own_rows], axis=0).reshape(
            blocks + 1, span_len, kv_local, HD
        )
        return jnp.concatenate([extended[:-1], extended[1:]], axis=1)

    key_band = make_band(k_heads, earlier[0])
    value_band = make_band(v_heads, earlier[1])
    query_blocks = q_heads.reshape(blocks, span_len, kv_local, group_size, HD)
    scores = jnp.einsum(
        "nqhgd,nkhd->nhgqk", query_blocks, key_band, preferred_element_type=jnp.float32
    ) * HD ** (-0.5)
    first_row = lax.axis_index("ep") * row_count
    query_index = jnp.arange(span_len, dtype=jnp.int32)[:, None]
    key_index = jnp.arange(2 * span_len, dtype=jnp.int32)[None, :]
    distance = query_index + span_len - key_index
    key_place = (
        first_row
        + jnp.arange(blocks, dtype=jnp.int32)[:, None, None] * span_len
        + key_index[None]
        - span_len
    )
    allowed = (distance >= 0)[None] & (distance < span_len)[None] & (key_place >= 0)
    masked = jnp.where(allowed[:, None, None], scores, -1e30)
    sink_full = sink_logits.reshape(kv_local, group_size)[None, :, :, None]
    row_max = jnp.maximum(jnp.max(masked, axis=-1), sink_full)
    weights_exp = jnp.exp(masked - row_max[..., None])
    denominator = jnp.sum(weights_exp, axis=-1) + jnp.exp(sink_full - row_max)
    probs = (weights_exp / denominator[..., None]).astype(jnp.bfloat16)
    attended = jnp.einsum(
        "nhgqk,nkhd->nqhgd", probs, value_band, preferred_element_type=jnp.float32
    )
    attended = attended.astype(jnp.bfloat16).reshape(row_count, kv_local * group_size * HD)
    mixed = jnp.dot(
        lax.all_gather(attended, "tp", axis=1, tiled=True),
        out_weight,
        preferred_element_type=jnp.float32,
    )
    mixer_out = mixed.astype(jnp.bfloat16)
    tp_count = lax.axis_size("tp")
    tp_index = lax.axis_index("tp")
    exp_local = expert_gate.shape[0]
    expert_count = exp_local * lax.axis_size("ep")
    rows_dev = tokens_b.shape[0] // tp_count
    capacity = min(4 * rows_dev // expert_count, rows_dev // 4)
    own_routes = lax.dynamic_slice_in_dim(route_expert, tp_index * rows_dev, rows_dev, 0)
    own_normed = normalize(
        lax.dynamic_slice_in_dim(tokens_b, tp_index * rows_dev, rows_dev, 0), moe_gain
    )
    flat_routes, places = slot_positions(own_routes, 1, expert_count)
    buffer = fill_slots(own_normed, flat_routes, places, 1, expert_count, capacity, exp_local)
    delivered = lax.all_to_all(buffer, "ep", split_axis=0, concat_axis=0, tiled=True)
    arrived = lax.all_gather(delivered, "tp", axis=2, tiled=True)
    own_flat = flat_routes[0]
    own_places = places[0]
    gates = gate_weights(own_normed, own_routes, router_group, router_expert)
    gate_pre = jnp.einsum(
        "setcd,edf->setcf", arrived, expert_gate, preferred_element_type=jnp.float32
    )
    up_pre = jnp.einsum("setcd,edf->setcf", arrived, expert_up, preferred_element_type=jnp.float32)
    activated = (jax.nn.silu(gate_pre) * up_pre).astype(jnp.bfloat16)
    partial_value = jnp.einsum(
        "setcf,efd->setcd", activated, expert_down, preferred_element_type=jnp.float32
    )
    summed = lax.psum_scatter(
        partial_value.astype(jnp.bfloat16), "tp", scatter_dimension=2, tiled=True
    )
    returned = lax.all_to_all(summed, "ep", split_axis=0, concat_axis=0, tiled=True)
    returned = returned.reshape(expert_count * capacity, returned.shape[-1])
    picked_rows = returned[own_flat * capacity + own_places].reshape(
        rows_dev, 2, returned.shape[-1]
    )
    moe_out = jnp.sum(gates[:, :, None] * picked_rows.astype(jnp.float32), axis=1).astype(
        jnp.bfloat16
    )
    return (mixer_out, moe_out)


def solution(mesh):
    in_specs = (
        P("ep", "tp"),
        P("ep", "tp"),
        P("ep", "tp"),
        P("tp"),
        P(None, "tp"),
        P("ep", None),
        P(),
        P(),
        P(),
        P("ep", None),
        P("ep", None, "tp"),
        P("ep", None, "tp"),
        P("ep", "tp", None),
    )
    out_specs = (P("ep", "tp"), P(("ep", "tp"), None))
    return jax.shard_map(
        per_device, mesh=mesh, in_specs=in_specs, out_specs=out_specs, check_vma=False
    )
```

```python
import contextlib
import functools

import jax
import jax.numpy as jnp
from jax import lax
from jax.experimental import pallas as pl
from jax.experimental.pallas import tpu as pltpu
from jax.sharding import PartitionSpec as P

HEADS = 16
KV = 4
HD = 64
WINDOW = 128


def shifted(value, axis, steps):
    count = lax.axis_size(axis)
    leading, last = (max(0, -steps), min(count, count - steps))
    return lax.ppermute(value, axis, [(source, source + steps) for source in range(leading, last)])


def normalize(rows_in, gain):
    values = rows_in.astype(jnp.float32)
    scaled = values * lax.rsqrt(jnp.mean(values * values, axis=-1, keepdims=True) + 1e-06) * gain
    return scaled.astype(jnp.bfloat16)


def gate_weights(normed, routes, router_group, router_expert):
    group_logits = jnp.dot(normed, router_group, preferred_element_type=jnp.float32)
    expert_logits = jnp.dot(normed, router_expert, preferred_element_type=jnp.float32)
    group_count = router_group.shape[1]
    expert_count = router_expert.shape[1]
    chosen_group = routes[:, 0] // (expert_count // group_count)
    group_match = chosen_group[:, None] == jnp.arange(group_count, dtype=jnp.int32)[None, :]
    group_share = jnp.sum(
        jnp.where(group_match, jax.nn.softmax(group_logits, axis=-1), 0.0), axis=-1
    )
    expert_match = routes[:, :, None] == jnp.arange(expert_count, dtype=jnp.int32)[None, None, :]
    picked = jnp.sum(jnp.where(expert_match, expert_logits[:, None, :], 0.0), axis=-1)
    return group_share[:, None] * jax.nn.softmax(picked, axis=-1)


def slot_positions(routes, sub_count, expert_count):
    flat_routes = routes.reshape(sub_count, -1)
    onehot = (
        flat_routes[:, :, None] == jnp.arange(expert_count, dtype=jnp.int32)[None, None, :]
    ).astype(jnp.int32)
    places = jnp.sum(onehot * jnp.cumsum(onehot, axis=1), axis=2) - 1
    return (flat_routes, places)


def fill_slots(normed, flat_routes, places, sub_count, expert_count, capacity, exp_local):
    sub_index = jnp.arange(sub_count, dtype=jnp.int32)[:, None]
    target = ((flat_routes * sub_count + sub_index) * capacity + places).reshape(-1)
    source = jnp.repeat(normed, 2, axis=0)
    buffer = jnp.zeros((expert_count * sub_count * capacity, normed.shape[1]), jnp.bfloat16)
    buffer = buffer.at[target].set(source)
    return buffer.reshape(
        expert_count // exp_local, exp_local, sub_count, capacity, normed.shape[1]
    )


LANES = 128
MESH = pl.DeviceIdType.MESH


@contextlib.contextmanager
def NS(name):
    pl.delay(1)
    yield
    pl.delay(1)

FIRST = "0"
SENDERS = 20
RECEIVERS = 56


def UNITS(chunk):
    half = chunk // 2
    return {
        "0": (0, 0, chunk),
        "1": (1, 0, chunk),
        "c": (2, 0, half),
        "d": (2, half, half),
        "a": (3, 0, half),
        "b": (3, half, half),
    }


def fused_kernel(
    groups,
    sink_hbm,
    q_hbm,
    k_hbm,
    v_hbm,
    gain_hbm,
    group_hbm,
    expert_hbm,
    route_hbm,
    tokens_hbm,
    gate_hbm,
    up_hbm,
    down_hbm,
    proj_hbm,
    mixed,
    back,
    take_out,
    sink_ref,
    q_ref,
    gain_ref,
    group_ref,
    expert_ref,
    route_ref,
    k_ext,
    v_ext,
    tokens,
    xs_ref,
    share_ref,
    heads,
    rows,
    part,
    wg,
    wu,
    wd,
    proj,
    act,
    from_core,
    relay_x,
    relay_y,
    from_xy,
    total,
    load_sem,
    out_sem,
    send_sem,
    recv_sem,
):
    ep, tp = lax.axis_index("ep"), lax.axis_index("tp")
    group, member = ep // 2, ep % 2
    x, core = tp // 2, tp % 2
    tp_x, tp_c = (1 - x) * 2 + core, x * 2 + (1 - core)
    ep_y = group * 2 + (1 - member)
    ep_count = groups * 2
    x_dev, y_dev, c_dev, d_dev = (ep, tp_x), (ep_y, tp), (ep, tp_c), (ep_y, tp_x)
    next_dev = ((ep + 1) % ep_count, tp)
    prev_dev = ((ep + ep_count - 1) % ep_count, tp)
    depth = back.shape[1]
    block = xs_ref.shape[0]
    chunk = block // groups
    row_count = q_ref.shape[0]
    mine, other = core * 4, (1 - core) * 4
    own = mine + member * 2 + x
    slot_x = mine + member * 2 + (1 - x)
    slot_y = mine + (1 - member) * 2 + x
    slot_d = mine + (1 - member) * 2 + (1 - x)
    mine_slots, other_slots = pl.ds(mine, 4), pl.ds(other, 4)

    def plane(step):
        return (group + step) % groups

    barrier = pltpu.get_barrier_semaphore()
    ahead = [plane(step) * 2 + member for step in range(1, groups)]
    peers = [(there, tp) for there in ahead] + [x_dev, y_dev, c_dev, d_dev, next_dev, prev_dev]
    for peer in peers:
        pl.semaphore_signal(barrier, inc=1, device_id=peer, device_id_type=MESH)

    first = pl.multiple_of(tp * block, block)
    inner = pl.ds(WINDOW, row_count)
    pairs = (
        (tokens_hbm.at[pl.ds(first, block)], tokens),
        (gain_hbm, gain_ref),
        (group_hbm, group_ref),
        (expert_hbm, expert_ref),
        (route_hbm.at[:, pl.ds(first, block)], route_ref),
        (k_hbm, k_ext.at[:, inner]),
        (v_hbm, v_ext.at[:, inner]),
        (q_hbm, q_ref),
        (sink_hbm, sink_ref),
        (gate_hbm, wg),
        (up_hbm, wu),
        (down_hbm, wd),
        (proj_hbm, proj),
    )
    loads = [
        pltpu.make_async_copy(source, held, load_sem.at[i])
        for i, (source, held) in enumerate(pairs)
    ]
    early, middle, late = loads[:5], loads[5:9], loads[9:]
    for load in early:
        load.start()
    early[4].wait()
    routes = route_ref[...]
    route_a, route_b = routes[0:1], routes[1:2]
    group_experts = expert_ref.shape[0] // groups
    group_at = lax.broadcasted_iota(jnp.int32, (groups, block), 0)
    inside = route_a - group_at * group_experts
    named = (inside >= 0) & (inside < group_experts)
    row_at = lax.broadcasted_iota(jnp.int32, (block, block), 0)
    column_at = lax.broadcasted_iota(jnp.int32, (block, block), 1)
    earlier = jnp.where(row_at < column_at, 1.0, 0.0).astype(jnp.bfloat16)
    counts = jnp.dot(
        jnp.where(named, 1.0, 0.0).astype(jnp.bfloat16), earlier, preferred_element_type=jnp.float32
    )
    first_row = (group_at * chunk).astype(jnp.float32)
    place = jnp.sum(jnp.where(named, counts + first_row, 0.0), axis=0, keepdims=True)
    take = jnp.where(row_at.astype(jnp.float32) == place, 1.0, 0.0).astype(jnp.bfloat16)
    with NS("wearly"):
        for load in early[:4]:
            load.wait()
    for load in middle + late:
        load.start()
    values = tokens[...].astype(jnp.float32)
    scale = lax.rsqrt(jnp.mean(values * values, axis=1, keepdims=True) + 1e-06)
    normed = (values * scale * gain_ref[...]).astype(jnp.bfloat16)
    across = (((1,), (1,)), ((), ()))
    xs_ref[...] = jnp.dot(take, normed, preferred_element_type=jnp.float32).astype(jnp.bfloat16)
    take_out[...] = take
    with NS("barrier"):
        pl.semaphore_wait(barrier, len(peers))

    in_flight, used, names = {}, [0], {}

    def descriptor(source, target, device, sender, name):
        receiver = names.setdefault(name, len(names))
        return pltpu.make_async_remote_copy(
            src_ref=source,
            dst_ref=target,
            send_sem=send_sem.at[sender],
            recv_sem=recv_sem.at[receiver],
            device_id=device,
            device_id_type=MESH,
        )

    def send(name, source, target, device):
        sender = used[0] % send_sem.shape[0]
        used[0] += 1
        if sender in in_flight:
            in_flight[sender].wait_send()
        copy = descriptor(source, target, device, sender, name)
        copy.start()
        in_flight[sender] = copy

    def receive(name, target, scope=None):
        with NS(scope or "w" + name):
            descriptor(target, target, x_dev, 0, name).wait_recv()

    my_start = pl.multiple_of(group * chunk, chunk)
    units = UNITS(chunk)
    piece_rows = 16
    near_pair = pl.ds(mine + member * 2, 2)
    far_pair = pl.ds(mine + (1 - member) * 2, 2)
    width_half = depth // 2
    sides = (pl.ds(0, width_half), pl.ds(width_half, width_half))

    def span_of(u):
        return pl.ds(units[u][1], units[u][2])

    def own_rows(s, begin, count):
        if s == 0:
            return xs_ref.at[pl.ds(pl.multiple_of(my_start + begin, piece_rows), count)]
        return rows.at[s, own, pl.ds(begin, count)]

    def depart(u):
        s, begin, count = units[u]
        if s:
            there = pl.ds(pl.multiple_of(plane(s) * chunk + begin, piece_rows), count)
            send(f"z{u}", xs_ref.at[there], rows.at[s, own, span_of(u)], (plane(s) * 2 + member, tp))

    def arrive(u):
        s = units[u][0]
        receive(f"z{u}", rows.at[s, own, span_of(u)])

    def gather_x(u):
        for i in range(units[u][2] // piece_rows):
            gather_piece(u, i)

    def gather_piece(u, i):
        s, begin, count = units[u]
        at = begin + i * piece_rows
        target = rows.at[s, own, pl.ds(at, piece_rows)]
        send(f"x{u}{i}", own_rows(s, at, piece_rows), target, x_dev)

    def gather_y(u):
        s, begin, count = units[u]
        send(f"y{u}", own_rows(s, begin, count), rows.at[s, own, span_of(u)], y_dev)

    def relay(u, i):
        s, begin, count = units[u]
        block_at = rows.at[s, slot_x, pl.ds(begin + i * piece_rows, piece_rows)]
        receive(f"x{u}{i}", block_at)
        send(f"y{u}", block_at, block_at, y_dev)

    def core_near(u):
        s = units[u][0]
        pair = rows.at[s, near_pair, span_of(u)]
        send(f"core{u}", pair, pair, c_dev)

    def core_far(u):
        s = units[u][0]
        pair = rows.at[s, far_pair, span_of(u)]
        receive(f"y{u}", pair)
        send(f"core{u}", pair, pair, c_dev)

    def up(u, e):
        s, begin, count = units[u]
        if e == 0:
            receive(f"core{u}", rows.at[s, other_slots, span_of(u)])
        batch = 8 * count
        with NS(f"up{u}{e}"):
            tokens = rows[s, :, begin : begin + count].reshape(batch, depth)
            held = share_ref[s].astype(jnp.float32)
            at = lax.broadcasted_iota(jnp.int32, held.shape, 1) % group_experts
            wanted = at == member * wg.shape[0] + e
            by_lane = jnp.sum(jnp.where(wanted, held, 0.0), axis=1, keepdims=True)
            shape = (8, count, block)
            lane = lax.broadcasted_iota(jnp.int32, shape, 2) - group * chunk - begin
            picked = lane == lax.broadcasted_iota(jnp.int32, shape, 1)
            share = jnp.sum(
                jnp.where(picked, jnp.broadcast_to(by_lane, shape), 0.0), axis=2, keepdims=True
            ).reshape(batch, 1)
            pre = jnp.dot(tokens, wg[e], preferred_element_type=jnp.float32)
            high = jnp.dot(tokens, wu[e], preferred_element_type=jnp.float32)
            act[e, :batch] = (jax.nn.silu(pre) * high * share).astype(jnp.bfloat16)

    def down(u):
        s, begin, count = units[u]
        batch = 8 * count
        tile = 512
        acts = jnp.concatenate([act[e, :batch] for e in range(wg.shape[0])], axis=1)

        def column(n, carry):
            columns = pl.ds(pl.multiple_of(n * tile, tile), tile)
            value = jnp.dot(acts, wd[:, columns], preferred_element_type=jnp.float32)
            part[s, :, begin : begin + count, columns] = value.astype(jnp.bfloat16).reshape(
                8, count, tile
            )
            return carry

        with NS(f"down{u}"):
            for i, side in enumerate(sides):
                tiles = width_half // tile
                lax.fori_loop(i * tiles, (i + 1) * tiles, column, 0)
                send(
                    f"sum{u}",
                    part.at[s, other_slots, span_of(u), side],
                    from_core.at[s, :, span_of(u), side],
                    c_dev,
                )

    def experts(u):
        for e in range(wg.shape[0]):
            up(u, e)
        down(u)

    def add(index, term):
        part[index] = (part[index].astype(jnp.float32) + term.astype(jnp.float32)).astype(
            jnp.bfloat16
        )

    def scatter(u):
        scatter_far(u)
        scatter_near(u)

    def scatter_far(u):
        s, begin, count = units[u]
        span = span_of(u)
        left, right = sides
        receive(f"sum{u}", from_core.at[s, :, span])
        with NS(f"E{u}"):
            add((s, mine_slots, span), from_core[s, :, span])
        send(f"dy{u}", part.at[s, slot_d, span, left], relay_y.at[s, span], y_dev)
        send(f"dx{u}", part.at[s, slot_d, span, right], relay_x.at[s, span], x_dev)

    def scatter_near(u):
        s, begin, count = units[u]
        span = span_of(u)
        left, right = sides
        send(f"xy{u}", part.at[s, slot_x, span, right], from_xy.at[s, 0, span, right], x_dev)
        send(f"xy{u}", part.at[s, slot_y, span, left], from_xy.at[s, 1, span, left], y_dev)

    def scatter_relay(u):
        s, begin, count = units[u]
        span = span_of(u)
        left, right = sides
        receive(f"dy{u}", relay_y.at[s, span])
        add((s, slot_x, span, left), relay_y[s, span])
        send(f"xy{u}", part.at[s, slot_x, span, left], from_xy.at[s, 0, span, left], x_dev)
        receive(f"dx{u}", relay_x.at[s, span])
        add((s, slot_y, span, right), relay_x[s, span])
        send(f"xy{u}", part.at[s, slot_y, span, right], from_xy.at[s, 1, span, right], y_dev)

    def home(u):
        s, begin, count = units[u]
        span = span_of(u)
        receive(f"xy{u}", from_xy.at[s, :, span], f"wH{u}")
        summed = (
            part[s, own, span].astype(jnp.float32)
            + from_xy[s, 0, span].astype(jnp.float32)
            + from_xy[s, 1, span].astype(jnp.float32)
        ).astype(jnp.bfloat16)
        there = pl.ds(pl.multiple_of(my_start + begin, piece_rows), count)
        if s:
            total[s, span] = summed
            to = (group + groups - s) % groups
            send("home", total.at[s, span], back.at[there], (to * 2 + member, tp))
        else:
            back[there] = summed

    def settle():
        receive("home", back.at[pl.ds(0, block - chunk)])

    head_count = q_ref.shape[1] // HD
    query_at = lax.broadcasted_iota(jnp.int32, (WINDOW, 2 * WINDOW), 0)
    key_at = lax.broadcasted_iota(jnp.int32, (WINDOW, 2 * WINDOW), 1)
    distance = query_at + WINDOW - key_at
    near = (distance >= 0) & (distance < WINDOW)

    def attend(b, carry):
        start = pl.multiple_of(b * WINDOW, WINDOW)
        keys = k_ext[:, pl.ds(start, 2 * WINDOW)]
        band = v_ext[:, pl.ds(start, 2 * WINDOW)]
        queries = q_ref[pl.ds(start, WINDOW)]
        allowed = near & (key_at + (ep * row_count + b * WINDOW - WINDOW) >= 0)
        outs = []
        for h in range(head_count):
            query = queries[:, h * HD : (h + 1) * HD]
            scores = jnp.dot(query, keys, preferred_element_type=jnp.float32) * HD ** (-0.5)
            masked = jnp.where(allowed, scores, -1e30)
            sink = jnp.full((WINDOW, 1), sink_ref[h], jnp.float32)
            row_max = jnp.maximum(jnp.max(masked, axis=1, keepdims=True), sink)
            weights = jnp.exp(masked - row_max)
            denominator = jnp.sum(weights, axis=1, keepdims=True) + jnp.exp(sink - row_max)
            probs = (weights * (1.0 / denominator)).astype(jnp.bfloat16)
            outs.append(lax.dot_general(probs, band, across, preferred_element_type=jnp.float32))
        heads[tp, pl.ds(start, WINDOW)] = jnp.concatenate(outs, axis=1).astype(jnp.bfloat16)
        return carry

    def att(first_block, last_block):
        with NS(f"att{first_block}"):
            lax.fori_loop(first_block, last_block, attend, 0)

    blocks = row_count // WINDOW
    pieces = 4
    piece = row_count // pieces

    def send_heads(begin, end):
        span = pl.ds(begin * WINDOW, (end - begin) * WINDOW)
        send("heads_x", heads.at[tp, span], heads.at[tp, span], x_dev)

    def share_heads():
        send("heads", heads.at[tp], heads.at[tp], c_dev)

    def relay_heads():
        receive("heads_x", heads.at[tp_x])
        send("heads", heads.at[tp_x], heads.at[tp_x], c_dev)

    def await_heads():
        receive("heads", heads.at[pl.ds(0, 2)])

    def project(i):
        span = pl.ds(i * piece, piece)
        with NS(f"proj{i}"):
            joined = jnp.concatenate([heads[t, span] for t in range(4)], axis=1)
            mixed[span] = jnp.dot(joined, proj[...], preferred_element_type=jnp.float32).astype(
                jnp.bfloat16
            )

    gather_piece(FIRST, 0)
    gather_y(FIRST)
    depart("1")
    group_logits = lax.dot_general(
        group_ref[...], normed, across, preferred_element_type=jnp.float32
    )
    expert_logits = lax.dot_general(
        expert_ref[...], normed, across, preferred_element_type=jnp.float32
    )
    group_exp = jnp.exp(group_logits - jnp.max(group_logits, axis=0, keepdims=True))
    group_share = jnp.sum(jnp.where(named, group_exp, 0.0), axis=0, keepdims=True) / jnp.sum(
        group_exp, axis=0, keepdims=True
    )
    expert_at = lax.broadcasted_iota(jnp.int32, expert_logits.shape, 0)
    logit_a = jnp.sum(jnp.where(expert_at == route_a, expert_logits, 0.0), axis=0, keepdims=True)
    logit_b = jnp.sum(jnp.where(expert_at == route_b, expert_logits, 0.0), axis=0, keepdims=True)
    top = jnp.maximum(logit_a, logit_b)
    exp_a, exp_b = jnp.exp(logit_a - top), jnp.exp(logit_b - top)
    gate_a = group_share * (exp_a / (exp_a + exp_b))
    gate_b = group_share * (exp_b / (exp_a + exp_b))
    base = jnp.sum(jnp.where(named, group_at * group_experts, 0), axis=0, keepdims=True)
    slot_at = lax.broadcasted_iota(jnp.int32, (group_experts, block), 0)
    share_t = jnp.where(slot_at == route_a - base, gate_a, 0.0) + jnp.where(
        slot_at == route_b - base, gate_b, 0.0
    )
    coarse = share_t.astype(jnp.bfloat16)
    fine = (share_t - coarse.astype(jnp.float32)).astype(jnp.bfloat16)
    for i, piece_of in enumerate((coarse, fine)):
        share_ref[0, own, pl.ds(i * group_experts, group_experts)] = lax.dot_general(
            piece_of, take, across, preferred_element_type=jnp.float32
        ).astype(jnp.bfloat16)
    for step in range(1, groups):
        there = (plane(step) * 2 + member, tp)
        send("share_z", share_ref.at[0, own], share_ref.at[step, own], there)

    gather_piece(FIRST, 1)

    def spread_shares():
        receive("share_z", share_ref.at[pl.ds(1, groups - 1), own])
        mine_now = share_ref.at[:, own]
        for device in (d_dev, x_dev, y_dev):
            send("share", mine_now, mine_now, device)

    def swap_shares():
        receive("share", share_ref.at[:, pl.ds(mine, 3)])
        core_now = share_ref.at[:, mine_slots]
        send("share_c", core_now, core_now, c_dev)

    def take_shares():
        receive("share_c", share_ref.at[:, other_slots])

    with NS("wqkv"):
        for load in middle:
            load.wait()
    for name, ext in (("k", k_ext), ("v", v_ext)):
        send("halo", ext.at[:, pl.ds(row_count, WINDOW)], ext.at[:, pl.ds(0, WINDOW)], next_dev)
    keep = pltpu.make_async_copy(
        xs_ref.at[pl.ds(my_start, chunk)], rows.at[0, own], out_sem.at[0]
    )
    keep.start()

    def take_halo():
        receive("halo", k_ext.at[:, pl.ds(0, 2 * WINDOW)])

    def take_weights():
        with NS("loads"):
            for load in late:
                load.wait()

    att(2, 4)
    send_heads(2, 4)
    att(4, 6)
    depart("c")
    depart("d")
    relay("0", 0)
    relay("0", 1)
    att(6, 7)
    spread_shares()
    arrive("1")
    gather_x("1")
    gather_y("1")
    att(7, 8)
    att(1, 2)
    take_halo()
    att(0, 1)
    share_heads()
    take_weights()
    keep.wait()
    core_near("0")
    send_heads(4, 6)
    core_far("0")
    swap_shares()
    relay("1", 0)
    relay("1", 1)
    depart("a")
    depart("b")
    core_near("1")
    arrive("c")
    gather_x("c")
    gather_y("c")
    arrive("d")
    gather_x("d")
    gather_y("d")
    take_shares()
    up("0", 0)
    up("0", 1)
    relay("c", 0)
    core_near("c")
    relay("d", 0)
    core_near("d")
    arrive("a")
    gather_x("a")
    gather_y("a")
    arrive("b")
    gather_x("b")
    gather_y("b")
    send_heads(6, 8)
    send_heads(0, 2)
    core_far("1")
    down("0")
    up("1", 0)
    up("1", 1)
    down("1")
    relay("a", 0)
    core_near("a")
    core_far("c")
    relay("b", 0)
    core_near("b")
    core_far("d")
    scatter_far("1")
    scatter_near("1")
    up("c", 0)
    up("c", 1)
    down("c")
    core_far("a")
    up("d", 0)
    up("d", 1)
    core_far("b")
    scatter_far("c")
    down("d")
    scatter_relay("1")
    scatter_near("c")
    relay_heads()
    up("a", 0)
    up("a", 1)
    scatter_far("d")
    scatter_near("d")
    down("a")
    scatter_relay("c")
    up("b", 0)
    up("b", 1)
    scatter_far("a")
    scatter_near("a")
    down("b")
    await_heads()
    home("1")
    scatter_far("b")
    scatter_near("b")
    scatter_relay("d")
    project(0)
    home("c")
    scatter_far("0")
    project(1)
    project(3)
    scatter_relay("a")
    project(2)
    home("d")
    scatter_relay("b")
    scatter_near("0")
    home("a")
    scatter_relay("0")
    home("b")
    home("0")
    settle()
    with NS("wsend"):
        for copy in in_flight.values():
            copy.wait_send()


def store_kernel(mixed, back, take, mixer_hbm, out_hbm, moved, sem):
    mixer_copy = pltpu.make_async_copy(mixed, mixer_hbm, sem.at[0])
    mixer_copy.start()
    moved[...] = lax.dot_general(
        take[...], back[...], (((0,), (0,)), ((), ())), preferred_element_type=jnp.float32
    ).astype(jnp.bfloat16)
    out_copy = pltpu.make_async_copy(moved, out_hbm, sem.at[1])
    out_copy.start()
    mixer_copy.wait()
    out_copy.wait()


def store(mixed, back, take):
    anywhere = pl.BlockSpec(memory_space=pl.ANY)
    vmem = pl.BlockSpec(memory_space=pltpu.VMEM)
    return pl.pallas_call(
        store_kernel,
        out_shape=tuple(jax.ShapeDtypeStruct(v.shape, v.dtype) for v in (mixed, back)),
        in_specs=[anywhere, vmem, vmem],
        out_specs=(anywhere, anywhere),
        scratch_shapes=[pltpu.VMEM(back.shape, back.dtype), pltpu.SemaphoreType.DMA((2,))],
        compiler_params=pltpu.CompilerParams(vmem_limit_bytes=8 * 2**20),
    )(*(pltpu.with_memory_space_constraint(v, pltpu.VMEM) for v in (mixed, back, take)))


def fused(
    sinks,
    q_heads,
    k_heads,
    v_heads,
    gain,
    router_group,
    router_expert,
    routes,
    tokens_b,
    expert_gate,
    expert_up,
    expert_down,
    proj,
):
    groups = router_group.shape[1]
    block = tokens_b.shape[0] // 4
    experts, depth, hidden = expert_gate.shape
    row_count, head_width = q_heads.shape
    down = expert_down.reshape(experts * hidden, depth)
    chunk = block // groups
    bf16 = jnp.bfloat16
    anywhere = pl.BlockSpec(memory_space=pl.ANY)
    mixed, back, take = pl.pallas_call(
        functools.partial(fused_kernel, groups),
        out_shape=(
            pltpu.VMEM((row_count, proj.shape[1]), bf16),
            pltpu.VMEM((block, depth), bf16),
            pltpu.VMEM((block, block), bf16),
        ),
        in_specs=[anywhere] * 13,
        out_specs=(pl.BlockSpec(memory_space=pltpu.VMEM),) * 3,
        scratch_shapes=[
            pltpu.SMEM(sinks.shape, jnp.float32),
            pltpu.VMEM(q_heads.shape, bf16),
            pltpu.VMEM((1, depth), jnp.float32),
            pltpu.VMEM((groups, depth), bf16),
            pltpu.VMEM((router_expert.shape[1], depth), bf16),
            pltpu.VMEM((2, block), jnp.int32),
            pltpu.VMEM((HD, row_count + WINDOW), bf16),
            pltpu.VMEM((HD, row_count + WINDOW), bf16),
            pltpu.VMEM((block, depth), bf16),
            pltpu.VMEM((block, depth), bf16),
            pltpu.VMEM((groups, 8, 2 * (router_expert.shape[1] // groups), block), bf16),
            pltpu.VMEM((4, row_count, head_width), bf16),
            pltpu.VMEM((groups, 8, chunk, depth), bf16),
            pltpu.VMEM((groups, 8, chunk, depth), bf16),
            pltpu.VMEM(expert_gate.shape, bf16),
            pltpu.VMEM(expert_up.shape, bf16),
            pltpu.VMEM(down.shape, bf16),
            pltpu.VMEM(proj.shape, bf16),
            pltpu.VMEM((experts, 8 * chunk, hidden), bf16),
            pltpu.VMEM((groups, 4, chunk, depth), bf16),
            pltpu.VMEM((groups, chunk, depth // 2), bf16),
            pltpu.VMEM((groups, chunk, depth // 2), bf16),
            pltpu.VMEM((groups, 2, chunk, depth), bf16),
            pltpu.VMEM((groups, chunk, depth), bf16),
            pltpu.SemaphoreType.DMA((13,)),
            pltpu.SemaphoreType.DMA((1,)),
            pltpu.SemaphoreType.DMA((SENDERS,)),
            pltpu.SemaphoreType.DMA((RECEIVERS,)),
        ],
        cost_estimate=pl.CostEstimate(
            flops=20_000_000_000, bytes_accessed=20_000_000, transcendentals=0
        ),
        compiler_params=pltpu.CompilerParams(
            collective_id=0, has_side_effects=True, vmem_limit_bytes=40 * 2**20
        ),
    )(
        *(
            pltpu.with_memory_space_constraint(value, pltpu.HBM)
            for value in (
                sinks,
                q_heads,
                k_heads.T,
                v_heads.T,
                gain[None, :],
                router_group.T,
                router_expert.T,
                routes.T,
                tokens_b,
                expert_gate,
                expert_up,
                down,
                proj,
            )
        )
    )
    return store(mixed, back, take)


def per_device(
    q_heads,
    k_heads,
    v_heads,
    sink_logits,
    out_weight,
    tokens_b,
    moe_gain,
    router_group,
    router_expert,
    route_expert,
    expert_gate,
    expert_up,
    expert_down,
):
    groups = router_group.shape[1]
    if (lax.axis_size("ep"), lax.axis_size("tp"), k_heads.shape[1]) == (2 * groups, 4, HD):
        return fused(
            sink_logits,
            q_heads,
            k_heads,
            v_heads,
            moe_gain,
            router_group,
            router_expert,
            route_expert,
            tokens_b,
            expert_gate,
            expert_up,
            expert_down,
            out_weight,
        )
    span_len = WINDOW
    row_count = q_heads.shape[0]
    kv_local = k_heads.shape[1] // HD
    group_size = HEADS // KV
    blocks = row_count // span_len
    stacked = jnp.stack([k_heads[row_count - span_len :], v_heads[row_count - span_len :]])
    earlier = shifted(stacked, "ep", 1)

    def make_band(own_rows, prev_rows):
        extended = jnp.concatenate([prev_rows, own_rows], axis=0).reshape(
            blocks + 1, span_len, kv_local, HD
        )
        return jnp.concatenate([extended[:-1], extended[1:]], axis=1)

    key_band = make_band(k_heads, earlier[0])
    value_band = make_band(v_heads, earlier[1])
    query_blocks = q_heads.reshape(blocks, span_len, kv_local, group_size, HD)
    scores = jnp.einsum(
        "nqhgd,nkhd->nhgqk", query_blocks, key_band, preferred_element_type=jnp.float32
    ) * HD ** (-0.5)
    first_row = lax.axis_index("ep") * row_count
    query_index = jnp.arange(span_len, dtype=jnp.int32)[:, None]
    key_index = jnp.arange(2 * span_len, dtype=jnp.int32)[None, :]
    distance = query_index + span_len - key_index
    key_place = (
        first_row
        + jnp.arange(blocks, dtype=jnp.int32)[:, None, None] * span_len
        + key_index[None]
        - span_len
    )
    allowed = (distance >= 0)[None] & (distance < span_len)[None] & (key_place >= 0)
    masked = jnp.where(allowed[:, None, None], scores, -1e30)
    sink_full = sink_logits.reshape(kv_local, group_size)[None, :, :, None]
    row_max = jnp.maximum(jnp.max(masked, axis=-1), sink_full)
    weights_exp = jnp.exp(masked - row_max[..., None])
    denominator = jnp.sum(weights_exp, axis=-1) + jnp.exp(sink_full - row_max)
    probs = (weights_exp / denominator[..., None]).astype(jnp.bfloat16)
    attended = jnp.einsum(
        "nhgqk,nkhd->nqhgd", probs, value_band, preferred_element_type=jnp.float32
    )
    attended = attended.astype(jnp.bfloat16).reshape(row_count, kv_local * group_size * HD)
    mixed = jnp.dot(
        lax.all_gather(attended, "tp", axis=1, tiled=True),
        out_weight,
        preferred_element_type=jnp.float32,
    )
    mixer_out = mixed.astype(jnp.bfloat16)
    tp_count = lax.axis_size("tp")
    tp_index = lax.axis_index("tp")
    exp_local = expert_gate.shape[0]
    expert_count = exp_local * lax.axis_size("ep")
    rows_dev = tokens_b.shape[0] // tp_count
    capacity = min(4 * rows_dev // expert_count, rows_dev // 4)
    own_routes = lax.dynamic_slice_in_dim(route_expert, tp_index * rows_dev, rows_dev, 0)
    own_normed = normalize(
        lax.dynamic_slice_in_dim(tokens_b, tp_index * rows_dev, rows_dev, 0), moe_gain
    )
    flat_routes, places = slot_positions(own_routes, 1, expert_count)
    buffer = fill_slots(own_normed, flat_routes, places, 1, expert_count, capacity, exp_local)
    delivered = lax.all_to_all(buffer, "ep", split_axis=0, concat_axis=0, tiled=True)
    arrived = lax.all_gather(delivered, "tp", axis=2, tiled=True)
    own_flat = flat_routes[0]
    own_places = places[0]
    gates = gate_weights(own_normed, own_routes, router_group, router_expert)
    gate_pre = jnp.einsum(
        "setcd,edf->setcf", arrived, expert_gate, preferred_element_type=jnp.float32
    )
    up_pre = jnp.einsum("setcd,edf->setcf", arrived, expert_up, preferred_element_type=jnp.float32)
    activated = (jax.nn.silu(gate_pre) * up_pre).astype(jnp.bfloat16)
    partial_value = jnp.einsum(
        "setcf,efd->setcd", activated, expert_down, preferred_element_type=jnp.float32
    )
    summed = lax.psum_scatter(
        partial_value.astype(jnp.bfloat16), "tp", scatter_dimension=2, tiled=True
    )
    returned = lax.all_to_all(summed, "ep", split_axis=0, concat_axis=0, tiled=True)
    returned = returned.reshape(expert_count * capacity, returned.shape[-1])
    picked_rows = returned[own_flat * capacity + own_places].reshape(
        rows_dev, 2, returned.shape[-1]
    )
    moe_out = jnp.sum(gates[:, :, None] * picked_rows.astype(jnp.float32), axis=1).astype(
        jnp.bfloat16
    )
    return (mixer_out, moe_out)


def solution(mesh):
    in_specs = (
        P("ep", "tp"),
        P("ep", "tp"),
        P("ep", "tp"),
        P("tp"),
        P(None, "tp"),
        P("ep", None),
        P(),
        P(),
        P(),
        P("ep", None),
        P("ep", None, "tp"),
        P("ep", None, "tp"),
        P("ep", "tp", None),
    )
    out_specs = (P("ep", "tp"), P(("ep", "tp"), None))
    return jax.shard_map(
        per_device, mesh=mesh, in_specs=in_specs, out_specs=out_specs, check_vma=False
    )
```
